128 devices in a mesh: sp: 16 (over z, y), dp: 8 (over x, core).
Axes of the slice: x: 4, y: 4, z: 4, core: 2. Of those that a mesh axis runs over, the one named last changes fastest.
Arguments:
- residual: bfloat16 [8, 2048, 2048], P('dp', 'sp'), may hold values from -6 to 6
- query: bfloat16 [8, 2048, 1536], P('dp', 'sp'), may hold values from -64 to 64
- latent: bfloat16 [8, 2048, 256], P('dp', 'sp'), may hold values from -6 to 6
- rope_key: bfloat16 [8, 2048, 32], P('dp', 'sp'), may hold values from -64 to 64
- latent_gain: float32 [256], replicated, may hold values from 0.1 to 1.9
- query_gain: float32 [96], replicated, may hold values from 0.7 to 5.6
- key_gain: float32 [96], replicated, may hold values from 0.7 to 5.6
- key_weight: bfloat16 [256, 1024], replicated, may hold values from -0.375 to 0.375
- value_weight: bfloat16 [256, 1024], replicated, may hold values from -0.375 to 0.375
- mix_gain: float32 [1024], replicated, may hold values from 0.1 to 1.9
- out_weight: bfloat16 [1024, 2048], replicated, may hold values from -0.1875 to 0.1875
- ffn_gain: float32 [2048], replicated, may hold values from 0.1 to 1.9
- expert_choice: int32 [8, 2048, 2], P('dp', 'sp'), may hold values from 0 to 127, as said below
- group_prob: float32 [8, 2048], P('dp', 'sp'), may hold values from 0.25 to 1
- expert_prob: float32 [8, 2048, 2], P('dp', 'sp'), may hold values from 0.05 to 1
- gate_weight: bfloat16 [128, 2048, 512], P(('sp', 'dp')), may hold values from -0.125 to 0.125
- up_weight: bfloat16 [128, 2048, 512], P(('sp', 'dp')), may hold values from -0.125 to 0.125
- down_weight: bfloat16 [128, 512, 2048], P(('sp', 'dp')), may hold values from -0.25 to 0.25
Outputs:
- layer_out: bfloat16 [8, 2048, 2048], P('dp', 'sp')
The draws below stay inside these ranges and needn't reach their ends.
Inputs may be any that keep to these rules, and one draw needn't show every extreme that they name: `expert_choice`: A token's two experts differ and lie in one group of 32 consecutive expert numbers. In each aligned block of 128 tokens (the tokens of one device) no expert is named more than 4 times, and every expert of one group is named exactly 4 times in every block.
All inputs are finite; a program needn't handle non-finite values.
Results may differ from the reference program's by a relative error of at most 0.012.
The reference program's roundings to bfloat16 on the way count: a program that leaves them out, or rounds other values in their place, can miss the bound.
Values may be sent and summed in bfloat16 or wider, within the bound.
A program may use at most 64 MiB of HBM per device.

```python
import jax
import jax.numpy as jnp
from jax import lax

D = 2048
HEADS = 16
NOPE = 64
ROPE = 32
VDIM = 64
LATENT = 256
FF = 512
GROUPS = 4
TOP = 2
SPAN = 64
TOK_DEV = 128
QK = 96
LENGTH = 2048
BATCH = 8
EXPERTS = 128
EPG = 32
CAP = 4
N_SP = 16
N_DP = 8


def paired_rows(key):
    base_key = jax.random.fold_in(key, 11)
    query_key, rope_draw_key = jax.random.split(base_key, 2)
    query_all = jax.random.truncated_normal(query_key, -4.0, 4.0, (BATCH, LENGTH, HEADS, QK), jnp.float32)
    rope_all = jax.random.truncated_normal(rope_draw_key, -4.0, 4.0, (BATCH, LENGTH, ROPE), jnp.float32)
    return (query_all.reshape(BATCH, LENGTH, HEADS * QK), rope_all)


def draw_query(key, part):
    return paired_rows(key)[0].astype(jnp.bfloat16)


def draw_rope_key(key, part):
    return paired_rows(key)[1].astype(jnp.bfloat16)


def head_gains(key, salt):
    gain_key = jax.random.fold_in(key, salt)
    gains = jax.random.uniform(gain_key, (QK,), jnp.float32, 0.7, 1.3)
    return gains


def draw_query_gain(key, part):
    return head_gains(key, 21)


def draw_key_gain(key, part):
    return head_gains(key, 22)


def draw_expert_choice(key, part):
    base_key = jax.random.fold_in(key, 31)
    hot_key, block_key = jax.random.split(base_key)
    half_rows = TOK_DEV // 2
    block_total = BATCH * LENGTH // TOK_DEV
    hot_group = jax.random.randint(hot_key, (), 0, GROUPS)

    def one_block(sub_key):
        cut_key, offset_key, shift_key, order_key = jax.random.split(sub_key, 4)
        cuts = jnp.sort(jax.random.randint(cut_key, (2,), 0, half_rows + 1))
        position = jnp.arange(TOK_DEV, dtype=jnp.int32)
        rest_pos = position - half_rows
        other_index = (rest_pos >= cuts[0]).astype(jnp.int32) + (rest_pos >= cuts[1]).astype(jnp.int32)
        other_group = (hot_group + 1 + other_index) % GROUPS
        group_of = jnp.where(position < half_rows, hot_group, other_group)
        other_start = jnp.where(other_index == 0, half_rows, jnp.where(other_index == 1, half_rows + cuts[0], half_rows + cuts[1]))
        group_start = jnp.where(position < half_rows, 0, other_start)
        rank_in = position - group_start
        offsets = jax.random.randint(offset_key, (GROUPS,), 0, EPG)
        shifts = jax.random.randint(shift_key, (GROUPS,), 1, EPG)
        first_local = (rank_in + offsets[group_of]) % EPG
        second_local = (first_local + shifts[group_of]) % EPG
        pairs = jnp.stack([group_of * EPG + first_local, group_of * EPG + second_local], axis=-1)
        shuffle = jax.random.permutation(order_key, TOK_DEV)
        return pairs[shuffle]
    blocks = jax.vmap(one_block)(jax.random.split(block_key, block_total))
    return blocks.reshape(BATCH, LENGTH, TOP).astype(jnp.int32)


def shard_levels(rng, shape, cuts, smallest, largest):
    gain = 1.0
    for dim, shards_of in cuts:
        heights = jax.random.uniform(jax.random.fold_in(jax.random.fold_in(rng, 6), dim), (shards_of,), jnp.float32, smallest / len(cuts), largest / len(cuts))
        gain = gain * jnp.repeat(jnp.exp(heights), shape[dim] // shards_of).reshape((-1,) + (1,) * (len(shape) - 1 - dim))
    return gain


def noise(stream_key, shape, width, bound, shards=(), kind=jnp.bfloat16):
    values = width * jax.random.normal(stream_key, shape, jnp.float32)
    if shards:
        values = values * shard_levels(stream_key, shape, shards, -0.22, 0.18)
    return jnp.clip(values, -bound, bound).astype(kind)


def setup_inputs(seed: int = 0) -> dict:
    key_list = jax.random.split(jax.random.key(seed), 19)
    return {
        "residual": noise(key_list[0], (BATCH, LENGTH, D), 1.0, 6.0, ((0, 8), (1, 16))),
        "query": draw_query(jax.random.fold_in(key_list[18], 71), 0),
        "latent": noise(key_list[2], (BATCH, LENGTH, LATENT), 1.0, 6.0, ((0, 8), (1, 16))),
        "rope_key": draw_rope_key(jax.random.fold_in(key_list[18], 71), 0),
        "latent_gain": jnp.clip(1.0 + 0.18 * jax.random.normal(key_list[4], (LATENT,), jnp.float32), 0.1, 1.9),
        "query_gain": draw_query_gain(jax.random.fold_in(key_list[18], 71), 0),
        "key_gain": draw_key_gain(jax.random.fold_in(key_list[18], 71), 0),
        "key_weight": noise(key_list[7], (LATENT, HEADS * NOPE), LATENT ** -0.5, 0.375),
        "value_weight": noise(key_list[8], (LATENT, HEADS * VDIM), LATENT ** -0.5, 0.375),
        "mix_gain": jnp.clip(1.0 + 0.18 * jax.random.normal(key_list[9], (HEADS * VDIM,), jnp.float32), 0.1, 1.9),
        "out_weight": noise(key_list[10], (HEADS * VDIM, D), (HEADS * VDIM) ** -0.5, 0.1875),
        "ffn_gain": jnp.clip(1.0 + 0.18 * jax.random.normal(key_list[11], (D,), jnp.float32), 0.1, 1.9),
        "expert_choice": draw_expert_choice(jax.random.fold_in(key_list[18], 71), 0),
        "group_prob": jnp.clip(0.25 + 0.75 * jax.random.uniform(key_list[13], (BATCH, LENGTH), jnp.float32) ** shard_levels(key_list[13], (BATCH, LENGTH), ((0, 8), (1, 16)), -0.2, 0.2), 0.25, 1.0),
        "expert_prob": jnp.clip(0.05 + 0.95 * jax.random.uniform(key_list[14], (BATCH, LENGTH, TOP), jnp.float32) ** shard_levels(key_list[14], (BATCH, LENGTH, TOP), ((0, 8), (1, 16)), -0.2, 0.2), 0.05, 1.0),
        "gate_weight": noise(key_list[15], (EXPERTS, D, FF), D ** -0.5, 0.125, ((0, 128),)),
        "up_weight": noise(key_list[16], (EXPERTS, D, FF), D ** -0.5, 0.125, ((0, 128),)),
        "down_weight": noise(key_list[17], (EXPERTS, FF, D), FF ** -0.5, 0.25, ((0, 128),)),
    }


eps = 1e-06

def rms_scale(vector, gains):
    return vector * lax.rsqrt(lax.optimization_barrier(jnp.mean(vector * vector, axis=-1, keepdims=True)) + eps) * gains

def rotate(vector, phases):
    half_width = vector.shape[-1] // 2
    lower_half = vector[..., :half_width]
    upper_half = vector[..., half_width:]
    cos_table = jnp.cos(phases)
    sin_table = jnp.sin(phases)
    return jnp.concatenate([lower_half * cos_table - upper_half * sin_table, upper_half * cos_table + lower_half * sin_table], axis=-1)

def angles(offset, span_count, rope_width):
    position = (offset + jnp.arange(span_count, dtype=jnp.int32)).astype(jnp.float32)
    frequency = 10000.0 ** (-2.0 * jnp.arange(rope_width // 2, dtype=jnp.float32) / rope_width)
    return position[:, None] * frequency[None, :]

def head_vectors(nope_part, rope_part, gains, phases):
    normed_all = rms_scale(jnp.concatenate([nope_part, rope_part], axis=-1), gains)
    split_at = nope_part.shape[-1]
    turned = rotate(normed_all[..., split_at:], phases[:, None, :])
    return jnp.concatenate([normed_all[..., :split_at], turned], axis=-1).astype(jnp.bfloat16)

def attend_one(query_head, key_head, value_head):
    length = query_head.shape[0]
    blocks_count = max(4, length // 1024)
    block_rows = length // blocks_count
    score_scale = query_head.shape[-1] ** (-0.5)
    pieces = []
    for block_index in range(blocks_count):
        first_row = block_index * block_rows
        last_row = first_row + block_rows
        scores = jnp.dot(query_head[first_row:last_row], key_head[:last_row].T, preferred_element_type=jnp.float32) * score_scale
        query_pos = first_row + jnp.arange(block_rows, dtype=jnp.int32)
        key_pos = jnp.arange(last_row, dtype=jnp.int32)
        allowed = key_pos[None, :] // SPAN <= query_pos[:, None] // SPAN
        scores = jnp.where(allowed, scores, -1e+30)
        row_top = lax.optimization_barrier(jnp.max(scores, axis=-1, keepdims=True))
        raised = jnp.exp(scores - row_top)
        row_sum = lax.optimization_barrier(jnp.sum(raised, axis=-1))
        summed = jnp.dot(raised.astype(jnp.bfloat16), value_head[:last_row], preferred_element_type=jnp.float32)
        pieces.append((summed / row_sum[:, None]).astype(jnp.bfloat16))
    return jnp.concatenate(pieces, axis=0)

def reference(residual, query, latent, rope_key, latent_gain, query_gain, key_gain, key_weight, value_weight, mix_gain, out_weight, ffn_gain, expert_choice, group_prob, expert_prob, gate_weight, up_weight, down_weight):
    phases = angles(0, LENGTH, ROPE)
    raw_query = query.astype(jnp.float32).reshape(BATCH, LENGTH, HEADS, QK)
    queries = head_vectors(raw_query[..., :NOPE], raw_query[..., NOPE:], query_gain, phases)
    normed_latent = rms_scale(latent.astype(jnp.float32), latent_gain).astype(jnp.bfloat16)
    flat_latent = normed_latent.reshape(BATCH * LENGTH, LATENT)
    key_part = jnp.dot(flat_latent, key_weight, preferred_element_type=jnp.float32).astype(jnp.bfloat16)
    key_part = key_part.reshape(BATCH, LENGTH, HEADS, NOPE)
    values = jnp.dot(flat_latent, value_weight, preferred_element_type=jnp.float32).astype(jnp.bfloat16)
    values = values.reshape(BATCH, LENGTH, HEADS, VDIM)
    shared_rope = jnp.broadcast_to(rope_key.astype(jnp.float32)[:, :, None, :], (BATCH, LENGTH, HEADS, ROPE))
    keys = head_vectors(key_part.astype(jnp.float32), shared_rope, key_gain, phases)

    def arrange(array):
        return array.transpose(0, 2, 1, 3).reshape(BATCH * HEADS, LENGTH, array.shape[-1])

    def per_head(operands):
        return attend_one(operands[0], operands[1], operands[2])
    heads_out = lax.map(per_head, (arrange(queries), arrange(keys), arrange(values)))
    heads_out = heads_out.reshape(BATCH, HEADS, LENGTH, VDIM).transpose(0, 2, 1, 3).reshape(BATCH * LENGTH, HEADS * VDIM)
    mixed_in = rms_scale(heads_out.astype(jnp.float32), mix_gain).astype(jnp.bfloat16)
    stream = residual.reshape(BATCH * LENGTH, D).astype(jnp.float32) + jnp.dot(mixed_in, out_weight, preferred_element_type=jnp.float32)
    normed = rms_scale(stream, ffn_gain).astype(jnp.bfloat16)
    shares = expert_prob.reshape(BATCH * LENGTH, TOP)
    route_weight = group_prob.reshape(BATCH * LENGTH, 1) * shares / lax.optimization_barrier(jnp.sum(shares, axis=-1, keepdims=True))
    flat_choice = expert_choice.reshape(BATCH * LENGTH * TOP)
    flat_route = route_weight.reshape(BATCH * LENGTH * TOP)
    assignments = BATCH * LENGTH * TOP
    most_rows = CAP * N_SP * N_DP

    def serve_expert(running, operands):
        expert_id, gate_one, up_one, down_one = operands
        picked = jnp.nonzero(flat_choice == expert_id, size=most_rows, fill_value=assignments)[0].astype(jnp.int32)
        token_ids = picked // TOP
        rows_in = jnp.take(normed, token_ids, axis=0, mode='fill', fill_value=0)
        gate_act = jnp.dot(rows_in, gate_one, preferred_element_type=jnp.float32)
        upward = jnp.dot(rows_in, up_one, preferred_element_type=jnp.float32)
        hidden = (jax.nn.silu(gate_act) * upward).astype(jnp.bfloat16)
        expert_out = jnp.dot(hidden, down_one, preferred_element_type=jnp.float32).astype(jnp.bfloat16)
        weight_of = jnp.take(flat_route, picked, mode='fill', fill_value=0.0)
        running = running.at[token_ids].add(weight_of[:, None] * expert_out.astype(jnp.float32), mode='drop')
        return (running, None)
    start_sum = jnp.zeros((BATCH * LENGTH, D), jnp.float32)
    routed_sum, _ = lax.scan(serve_expert, start_sum, (jnp.arange(EXPERTS, dtype=jnp.int32), gate_weight, up_weight, down_weight))
    return (stream + routed_sum).astype(jnp.bfloat16).reshape(BATCH, LENGTH, D)
```

```python
import functools

import jax
import jax.numpy as jnp
import numpy as np
from jax import lax
from jax.experimental import pallas as pl
from jax.experimental.pallas import tpu as pltpu
from jax.sharding import PartitionSpec as P

GROUPS = 4
SPAN = 64


eps = 1e-06


def dot32(a, b):
    return jnp.dot(a, b, preferred_element_type=jnp.float32)


def dot_t(a, b):
    return lax.dot_general(a, b, (((0,), (0,)), ((), ())), preferred_element_type=jnp.float32)


def expert_kernel(
    n_y,
    n_dp,
    cap,
    rows,
    normed_ref,
    info_ref,
    pick_ref,
    stream_ref,
    gate_hbm,
    up_hbm,
    down_hbm,
    out_ref,
    gate_ref,
    up_ref,
    down_ref,
    out1,
    in1,
    out2,
    arrive,
    served,
    back2,
    merged,
    home,
    acc,
    w_sem,
    s1,
    r1,
    s2,
    r2,
    s3,
    r3,
    s4,
    r4,
    l_sem,
):
    peers = n_y * n_dp
    width = normed_ref.shape[1]
    sp = lax.axis_index("sp")
    dp = lax.axis_index("dp")
    plane = sp // n_y
    row = sp % n_y
    mine = row * n_dp + dp

    def column(k):
        return {"sp": ((plane + k) % GROUPS) * n_y + row, "dp": dp}

    def peer(j):
        other = (mine + j) % peers
        return {"sp": plane * n_y + other // n_dp, "dp": other % n_dp}

    loads = [
        pltpu.make_async_copy(gate_hbm, gate_ref, w_sem.at[0]),
        pltpu.make_async_copy(up_hbm, up_ref, w_sem.at[1]),
        pltpu.make_async_copy(down_hbm, down_ref, w_sem.at[2]),
    ]
    for load in loads:
        load.start()
    barrier = pltpu.get_barrier_semaphore()
    for k in range(1, GROUPS):
        pl.semaphore_signal(barrier, inc=1, device_id=column(k), device_id_type=pl.DeviceIdType.MESH)
    for j in range(1, peers):
        pl.semaphore_signal(barrier, inc=1, device_id=peer(j), device_id_type=pl.DeviceIdType.MESH)

    def remote(src, dst, send, recv, target):
        return pltpu.make_async_remote_copy(
            src_ref=src,
            dst_ref=dst,
            send_sem=send,
            recv_sem=recv,
            device_id=target,
            device_id_type=pl.DeviceIdType.MESH,
        )

    first = {}

    def pack(k, target):
        picks = pick_ref[(plane + k) % GROUPS]
        target[k, :, :width] = dot32(picks, normed_ref[...]).astype(jnp.bfloat16)
        target[k, :, width:] = dot32(picks, info_ref[...]).astype(jnp.bfloat16)

    for k in (2, 1, 3):
        pack(k, out1)
        if k == 2:
            pl.semaphore_wait(barrier, GROUPS - 1 + peers - 1)
        first[k] = remote(out1.at[k], in1.at[k], s1.at[k], r1.at[k], column(k))
        first[k].start()
    pack(0, in1)

    def slots(k):
        info = in1[k, :, width:].astype(jnp.float32)
        place = lax.broadcasted_iota(jnp.int32, (rows, peers * cap), 1).astype(jnp.float32)
        return place == info[:, 0:1], place == info[:, 1:2], info

    second = {}

    def scatter(k):
        if k:
            first[k].wait_recv()
        at0, at1, _ = slots(k)
        choose = (at0.astype(jnp.float32) + at1.astype(jnp.float32)).astype(jnp.bfloat16)
        placed = dot_t(choose, in1[k, :, :width]).astype(jnp.bfloat16)
        for e in range(peers):
            out2[k, e] = placed[e * cap : (e + 1) * cap]
        second[k] = [
            remote(
                out2.at[k, (mine + j) % peers], arrive.at[k, j], s2.at[k, j], r2.at[k, j], peer(j)
            )
            for j in range(1, peers)
        ]
        for copy in second[k]:
            copy.start()
        arrive[k, 0] = out2[k, mine]

    third = {}

    def serve(k):
        for copy in second[k]:
            copy.wait_recv()
        if k == 2:
            for load in loads:
                load.wait()
        given = arrive[k].reshape(peers * cap, width)
        gate_act = dot32(given, gate_ref[...])
        upward = dot32(given, up_ref[...])
        hidden = (gate_act * (1.0 / (1.0 + jnp.exp(-gate_act))) * upward).astype(jnp.bfloat16)
        result = dot32(hidden, down_ref[...]).astype(jnp.bfloat16)
        for j in range(peers):
            served[k, j] = result[j * cap : (j + 1) * cap]
        third[k] = [
            remote(
                served.at[k, j], back2.at[k, mine], s3.at[k, j], r3.at[k, peers - j], peer(peers - j)
            )
            for j in range(1, peers)
        ]
        for copy in third[k]:
            copy.start()
        back2[k, mine] = served[k, 0]

    fourth = {}

    def merge(k):
        for copy in third[k]:
            copy.wait_recv()
        at0, at1, info = slots(k)
        high = jnp.where(at0, info[:, 2:3], 0.0) + jnp.where(at1, info[:, 4:5], 0.0)
        low = jnp.where(at0, info[:, 3:4], 0.0) + jnp.where(at1, info[:, 5:6], 0.0)
        got = back2[k].reshape(peers * cap, width)
        total = dot32(high.astype(jnp.bfloat16), got) + dot32(low.astype(jnp.bfloat16), got)
        if k:
            merged[k] = total.astype(jnp.bfloat16)
            fourth[k] = remote(merged.at[k], home.at[k], s4.at[k], r4.at[k], column(GROUPS - k))
            fourth[k].start()
        else:
            acc[...] = stream_ref[...] + dot_t(pick_ref[plane], total.astype(jnp.bfloat16))

    scatter(0)
    scatter(2)
    scatter(1)
    scatter(3)
    serve(2)
    serve(1)
    serve(3)
    merge(2)
    merge(1)
    merge(3)
    serve(0)
    merge(0)
    for k in (2, 1, 3):
        fourth[k].wait_recv()
        acc[...] += dot_t(pick_ref[(plane + k) % GROUPS], home[k])
    out_ref[...] = acc[...].astype(jnp.bfloat16)
    for k in range(GROUPS):
        if k:
            first[k].wait_send()
            fourth[k].wait_send()
        for copy in second[k] + third[k]:
            copy.wait_send()


def attention_kernel(
    n_sp,
    n_y,
    nope,
    rope,
    value_width,
    query_hbm,
    latent_ref,
    rope_t_ref,
    latent_gain_ref,
    gains_ref,
    near_ref,
    far_ref,
    mix_gain_ref,
    ffn_gain_ref,
    residual_hbm,
    key_weight_hbm,
    value_weight_hbm,
    out_weight_hbm,
    stream_ref,
    normed_ref,
    residual_ref,
    key_weight_ref,
    value_weight_ref,
    out_weight_ref,
    wide_key,
    pick_query,
    turn_query,
    queries_in,
    packed,
    packed_in,
    queries,
    keys,
    values,
    bias,
    weights,
    heads_out,
    token_in,
    w_sem,
    sq,
    rq,
    sz,
    rz,
    sy,
    ry,
    so,
    ro,
):
    bf = jnp.bfloat16
    f32 = jnp.float32
    tok = latent_ref.shape[0]
    lat = latent_ref.shape[1]
    qk = nope + rope
    half = rope // 2
    n_z = n_sp // n_y
    heads = n_z
    slot = 128
    wide_q = heads * qk
    wide_v = heads * value_width
    me = lax.axis_index("sp")
    z = me // n_y
    y = me % n_y

    def local(src, dst, k):
        return pltpu.make_async_copy(src, dst, w_sem.at[k])

    def query_part(target):
        return query_hbm.at[:, pl.ds(pl.multiple_of(target * wide_q, slot), wide_q)]

    own_part = pl.ds(pl.multiple_of(z * wide_v, slot), wide_v)
    loads = [
        local(key_weight_hbm.at[:, own_part], key_weight_ref, 0),
        local(value_weight_hbm.at[:, own_part], value_weight_ref, 1),
        local(query_part(z), queries_in.at[z], 2),
        local(residual_hbm, residual_ref, 3),
        local(out_weight_hbm, out_weight_ref, 4),
    ]
    for load in loads:
        load.start()

    def remote(src, dst, send, recv, target):
        return pltpu.make_async_remote_copy(
            src_ref=src,
            dst_ref=dst,
            send_sem=send,
            recv_sem=recv,
            device_id={"sp": target},
            device_id_type=pl.DeviceIdType.MESH,
        )

    def at_z(k):
        return ((z + k) % n_z) * n_y + y

    def at_y(m):
        return z * n_y + (y + m) % n_y

    barrier = pltpu.get_barrier_semaphore()
    for target in [at_z(k) for k in range(1, n_z)] + [at_y(m) for m in range(1, n_y)]:
        pl.semaphore_signal(
            barrier, inc=1, device_id={"sp": target}, device_id_type=pl.DeviceIdType.MESH
        )
    raw = latent_ref[...].astype(f32)
    scale = lax.rsqrt(jnp.mean(raw * raw, axis=-1, keepdims=True) + eps)
    packed[:tok] = (raw * scale * latent_gain_ref[...]).astype(bf)
    packed[tok:, :tok] = rope_t_ref[:half]
    packed[tok:, tok:] = rope_t_ref[half:]
    pl.semaphore_wait(barrier, n_z - 1 + n_y - 1)

    sent = []
    down = {}
    for k in (1, 3, 2):
        down[k] = remote(packed, packed_in.at[me], sz.at[k], rz.at[k], at_z(k))
        down[k].start()

    def spread(k, source):
        index = ((z + n_z - k) % n_z) * n_y + y
        for m in (1, 3, 2):
            sent.append(remote(source, packed_in.at[index], sy.at[k, m], ry.at[k, m], at_y(m)))
            sent[-1].start()

    spread(0, packed)
    asked = []
    for k in (1, 3, 2):
        target = (z + k) % n_z
        asked.append(remote(query_part(target), queries_in.at[z], sq.at[k], rq.at[k], at_z(k)))
        asked[-1].start()

    packed_in[me] = packed[...]

    def selector(rows, columns, source):
        i = lax.broadcasted_iota(jnp.int32, (rows, columns), 0)
        c = lax.broadcasted_iota(jnp.int32, (rows, columns), 1)
        return (i == source(c // slot, c % slot)).astype(f32).astype(bf)

    def swapped(c):
        return jnp.where(
            c < nope, -1, jnp.where(c < nope + half, c + half, jnp.where(c < qk, c - half, -1))
        )

    def plain_of(c, first):
        return jnp.where((c >= first) & (c < qk), c, -1)

    pick_query[...] = selector(
        wide_q, heads * slot, lambda h, c: jnp.where(c < qk, c + h * qk, -1)
    )
    turn_query[...] = selector(
        wide_q,
        heads * slot,
        lambda h, c: jnp.where((c >= nope) & (c < qk), swapped(c) + h * qk, -1),
    )
    pick_rope = selector(
        rope,
        2 * slot,
        lambda h, c: jnp.where(
            (c < nope) | (c >= qk), -1, jnp.where(h == 0, c, swapped(c)) - nope
        ),
    )
    q_pos = y * tok + lax.broadcasted_iota(jnp.int32, bias.shape, 0)
    k_pos = lax.broadcasted_iota(jnp.int32, bias.shape, 1)
    bias[...] = jnp.where(k_pos // SPAN <= q_pos // SPAN, 0.0, -1e30)
    loads[0].wait()
    wide_key[...] = dot32(
        key_weight_ref[...],
        selector(heads * nope, heads * slot, lambda h, c: jnp.where(c < nope, c + h * nope, -1)),
    ).astype(bf)
    loads[1].wait()

    for k in (1, 3, 2):
        down[k].wait_recv()
        spread(k, packed_in.at[((z + n_z - k) % n_z) * n_y + y])

    near_cos, near_sin = near_ref[0], near_ref[1]

    def tables(block):
        far_cos = far_ref[0, pl.ds(block, 1), :]
        far_sin = far_ref[1, pl.ds(block, 1), :]
        return (
            far_cos * near_cos - far_sin * near_sin,
            far_sin * near_cos + far_cos * near_sin,
        )

    query_gain, query_swap = gains_ref[0:1, :], gains_ref[1:2, :]
    key_gain, key_swap = gains_ref[2:3, :], gains_ref[3:4, :]

    def prepare(i, carry):
        step = i // n_y
        k = jnp.where(step < 2, step, 5 - step)
        m = i % n_y
        origin = (z + n_z - k) % n_z
        s = origin * n_y + (y + n_y - m) % n_y

        @pl.when(m > 0)
        def _():
            remote(packed, packed_in.at[s], sy.at[k, m], ry.at[k, m], me).wait_recv()

        rows = pl.ds(pl.multiple_of(s * tok, tok), tok)
        block = packed_in[s]
        latent = block[:tok]
        values[rows, :] = dot32(latent, value_weight_ref[...]).astype(bf)
        part = dot32(latent, wide_key[...]).astype(bf).astype(f32)
        turned_rows = jnp.concatenate([block[tok:, :tok], block[tok:, tok:]], axis=0)
        spun = dot_t(turned_rows, pick_rope)
        cos, sin = tables(s)
        plain_rope = spun[:, :slot]
        tail = plain_rope * (key_gain * cos) + spun[:, slot:] * (key_swap * sin)
        for h in range(heads):
            own = part[:, h * slot : (h + 1) * slot]
            full = own + plain_rope
            norm = lax.rsqrt(jnp.sum(full * full, axis=-1, keepdims=True) / qk + eps)
            keys[h, rows, :] = ((own * key_gain + tail) * norm).astype(bf)
        return carry

    lax.fori_loop(0, n_sp, prepare, 0)

    loads[2].wait()
    for copy in asked:
        copy.wait_recv()

    def prepare_queries(b, carry):
        raw = queries_in[b]
        plain = dot32(raw, pick_query[...])
        turned = dot32(raw, turn_query[...])
        cos, sin = tables(b * n_y + y)
        for h in range(heads):
            span = slice(h * slot, (h + 1) * slot)
            own = plain[:, span]
            norm = lax.rsqrt(jnp.sum(own * own, axis=-1, keepdims=True) / qk + eps)
            queries[b, h] = (
                (own * (query_gain * cos) + turned[:, span] * (query_swap * sin)) * norm
            ).astype(bf)
        return carry

    lax.fori_loop(0, n_z, prepare_queries, 0)

    stretch = n_y * tok
    factor = qk ** (-0.5) * 1.4426950408889634
    lane = lax.broadcasted_iota(jnp.int32, (tok, wide_v), 1) // value_width
    for b in range(n_z - 1, -1, -1):
        last = (b + 1) * stretch
        sums = []
        for h in range(heads):
            scores = lax.dot_general(
                queries[b, h],
                keys[h, :last],
                (((1,), (1,)), ((), ())),
                preferred_element_type=f32,
            )
            edge = scores[:, last - stretch :] + bias[...]
            top = jnp.max(edge, axis=-1, keepdims=True)
            if b:
                inner = scores[:, : last - stretch]
                top = jnp.maximum(top, jnp.max(inner, axis=-1, keepdims=True))
            raised = jnp.exp2((edge - top) * factor)
            total = jnp.sum(raised, axis=-1, keepdims=True)
            weights[h * tok : (h + 1) * tok, last - stretch : last] = raised.astype(bf)
            if b:
                raised = jnp.exp2((inner - top) * factor)
                total = total + jnp.sum(raised, axis=-1, keepdims=True)
                weights[h * tok : (h + 1) * tok, : last - stretch] = raised.astype(bf)
            sums.append(total)
        mixed = dot32(weights[:, :last], values[:last])
        total = None
        for h in range(heads):
            mine = mixed[h * tok : (h + 1) * tok] / sums[h]
            total = mine if total is None else jnp.where(lane < h, total, mine)
        heads_out[b] = total.astype(bf)

        @pl.when(z != b)
        def _():
            remote(
                heads_out.at[b], token_in.at[z], so.at[b], ro.at[z], b * n_y + y
            ).start()

    token_in[z] = heads_out[z]
    loads[3].wait()
    loads[4].wait()
    for k in range(1, n_z):
        other = (z + k) % n_z
        remote(
            heads_out.at[other], token_in.at[other], so.at[other], ro.at[other], other * n_y + y
        ).wait()
    square = None
    for s in range(n_z):
        piece = token_in[s].astype(f32)
        part = jnp.sum(piece * piece, axis=-1, keepdims=True)
        square = part if square is None else square + part
    scale = lax.rsqrt(square / (n_z * wide_v) + eps)
    mixed = jnp.concatenate(
        [
            (token_in[s].astype(f32) * scale * mix_gain_ref[:, s * wide_v : (s + 1) * wide_v]).astype(bf)
            for s in range(n_z)
        ],
        axis=1,
    )
    stream = residual_ref[...].astype(f32) + dot32(mixed, out_weight_ref[...])
    stream_ref[...] = stream
    scale = lax.rsqrt(jnp.mean(stream * stream, axis=-1, keepdims=True) + eps)
    normed_ref[...] = (stream * scale * ffn_gain_ref[...]).astype(bf)
    for copy in list(down.values()) + sent + asked:
        copy.wait_send()


def trig(positions, nope, rope):
    frequency = 10000.0 ** (-2.0 * np.arange(rope // 2) / rope)
    angle = np.asarray(positions, np.float64)[:, None] * frequency[None, :]
    cos = np.ones((len(positions), 128))
    sin = np.zeros((len(positions), 128))
    cos[:, nope : nope + rope] = np.concatenate([np.cos(angle)] * 2, axis=1)
    sin[:, nope : nope + rope] = np.concatenate([np.sin(angle)] * 2, axis=1)
    return np.stack([cos, sin]).astype(np.float32)


def attended(
    residual,
    query,
    latent,
    rope_key,
    latent_gain,
    query_gain,
    key_gain,
    key_weight,
    value_weight,
    mix_gain,
    out_weight,
    ffn_gain,
    head_count,
    nope,
    value_width,
):
    n_sp = lax.axis_size("sp")
    n_y = n_sp // GROUPS
    n_z = GROUPS
    tok, width = residual.shape
    rope = rope_key.shape[1]
    qk = nope + rope
    lat = latent.shape[1]
    heads = head_count // n_z
    length = n_sp * tok
    half = rope // 2
    bf = jnp.bfloat16
    slot = 128

    def both(gain):
        turned = jnp.concatenate([jnp.zeros((nope,)), -gain[nope + half :], gain[nope : nope + half]])
        return jnp.pad(jnp.stack([gain, turned]), ((0, 0), (0, slot - qk)))

    gains = jnp.concatenate([both(query_gain), both(key_gain)], axis=0)
    near = jnp.asarray(trig(np.arange(tok), nope, rope))
    far = jnp.asarray(trig(np.arange(n_sp) * tok, nope, rope))
    vmem = pl.BlockSpec(memory_space=pltpu.VMEM)
    hbm = pl.BlockSpec(memory_space=pl.ANY)
    dma = pltpu.SemaphoreType.DMA
    wide_v = heads * value_width
    return pl.pallas_call(
        functools.partial(attention_kernel, n_sp, n_y, nope, rope, value_width),
        out_shape=(
            jax.ShapeDtypeStruct((tok, width), jnp.float32),
            jax.ShapeDtypeStruct((tok, width), bf),
        ),
        in_specs=[hbm] + [vmem] * 8 + [hbm] * 4,
        out_specs=(vmem, vmem),
        scratch_shapes=[
            pltpu.VMEM((tok, width), bf),
            pltpu.VMEM((lat, wide_v), bf),
            pltpu.VMEM((lat, wide_v), bf),
            pltpu.VMEM(out_weight.shape, bf),
            pltpu.VMEM((lat, heads * slot), bf),
            pltpu.VMEM((heads * qk, heads * slot), bf),
            pltpu.VMEM((heads * qk, heads * slot), bf),
            pltpu.VMEM((n_z, tok, heads * qk), bf),
            pltpu.VMEM((tok + half, lat), bf),
            pltpu.VMEM((n_sp, tok + half, lat), bf),
            pltpu.VMEM((n_z, heads, tok, slot), bf),
            pltpu.VMEM((heads, length, slot), bf),
            pltpu.VMEM((length, wide_v), bf),
            pltpu.VMEM((tok, n_y * tok), jnp.float32),
            pltpu.VMEM((heads * tok, length), bf),
            pltpu.VMEM((n_z, tok, wide_v), bf),
            pltpu.VMEM((n_z, tok, wide_v), bf),
            dma((5,)),
            dma((n_z,)),
            dma((n_z,)),
            dma((n_z,)),
            dma((n_z,)),
            dma((n_z, n_y)),
            dma((n_z, n_y)),
            dma((n_z,)),
            dma((n_z,)),
        ],
        compiler_params=pltpu.CompilerParams(
            collective_id=1, has_side_effects=True, vmem_limit_bytes=48 * 1024 * 1024
        ),
    )(
        query,
        latent,
        rope_key.T,
        latent_gain[None],
        gains,
        near,
        far,
        mix_gain[None],
        ffn_gain[None],
        residual,
        key_weight,
        value_weight,
        out_weight,
    )


def routed(normed, stream, choice, group_prob, share, gate, up, down, expert_total):
    tok_rows, width = normed.shape
    n_y = lax.axis_size("sp") // GROUPS
    n_dp = lax.axis_size("dp")
    per_group = expert_total // GROUPS
    cap = tok_rows * GROUPS // expert_total
    rows = per_group * cap // choice.shape[1]
    group = choice[:, 0] // per_group
    order = jnp.arange(tok_rows, dtype=jnp.int32)
    before = order[None, :] < order[:, None]
    rank = jnp.sum((before & (group[None, :] == group[:, None])).astype(jnp.int32), axis=1)
    line = group * rows + rank
    pick = (
        (line[None, :] == jnp.arange(GROUPS * rows, dtype=jnp.int32)[:, None])
        .astype(jnp.bfloat16)
        .reshape(GROUPS, rows, tok_rows)
    )
    route = group_prob[:, None] * share / jnp.sum(share, axis=-1, keepdims=True)
    earlier = jnp.sum(
        (
            before[:, None, :, None] & (choice[:, :, None, None] == choice[None, None, :, :])
        ).astype(jnp.int32),
        axis=(2, 3),
    )
    position = (choice - group[:, None] * per_group) * cap + earlier
    high = lax.reduce_precision(route, 8, 7)
    low = route - high
    columns = jnp.concatenate(
        [
            position.astype(jnp.float32),
            jnp.stack([high[:, 0], low[:, 0], high[:, 1], low[:, 1]], axis=1),
            jnp.zeros((tok_rows, 122), jnp.float32),
        ],
        axis=1,
    ).astype(jnp.bfloat16)
    hidden = gate.shape[1]
    bf = jnp.bfloat16
    vmem = pl.BlockSpec(memory_space=pltpu.VMEM)
    hbm = pl.BlockSpec(memory_space=pl.ANY)
    dma = pltpu.SemaphoreType.DMA
    return pl.pallas_call(
        functools.partial(expert_kernel, n_y, n_dp, cap, rows),
        out_shape=jax.ShapeDtypeStruct((tok_rows, width), bf),
        in_specs=[vmem] * 4 + [hbm] * 3,
        out_specs=vmem,
        scratch_shapes=[
            pltpu.VMEM((width, hidden), bf),
            pltpu.VMEM((width, hidden), bf),
            pltpu.VMEM((hidden, width), bf),
            pltpu.VMEM((GROUPS, rows, width + 128), bf),
            pltpu.VMEM((GROUPS, rows, width + 128), bf),
            pltpu.VMEM((GROUPS, per_group, cap, width), bf),
            pltpu.VMEM((GROUPS, per_group, cap, width), bf),
            pltpu.VMEM((GROUPS, per_group, cap, width), bf),
            pltpu.VMEM((GROUPS, per_group, cap, width), bf),
            pltpu.VMEM((GROUPS, rows, width), bf),
            pltpu.VMEM((GROUPS, rows, width), bf),
            pltpu.VMEM((tok_rows, width), jnp.float32),
            dma((3,)),
            dma((GROUPS,)),
            dma((GROUPS,)),
            dma((GROUPS, per_group)),
            dma((GROUPS, per_group)),
            dma((GROUPS, per_group)),
            dma((GROUPS, per_group)),
            dma((GROUPS,)),
            dma((GROUPS,)),
            dma((1,)),
        ],
        compiler_params=pltpu.CompilerParams(
            collective_id=0, has_side_effects=True, vmem_limit_bytes=60 * 1024 * 1024
        ),
    )(normed, columns, pick, stream, gate, up, down)


def per_device(
    residual,
    query,
    latent,
    rope_key,
    latent_gain,
    query_gain,
    key_gain,
    key_weight,
    value_weight,
    mix_gain,
    out_weight,
    ffn_gain,
    expert_choice,
    group_prob,
    expert_prob,
    gate_weight,
    up_weight,
    down_weight,
):
    rope_width = rope_key.shape[2]
    qk_width = query_gain.shape[0]
    nope_width = qk_width - rope_width
    head_count = query.shape[2] // qk_width
    value_width = value_weight.shape[1] // head_count
    seq_devices = lax.axis_size("sp")
    stream, normed = attended(
        residual[0],
        query[0],
        latent[0],
        rope_key[0],
        latent_gain,
        query_gain,
        key_gain,
        key_weight,
        value_weight,
        mix_gain,
        out_weight,
        ffn_gain,
        head_count,
        nope_width,
        value_width,
    )
    expert_total = seq_devices * lax.axis_size("dp")
    return routed(
        normed,
        stream,
        expert_choice[0],
        group_prob[0],
        expert_prob[0],
        gate_weight[0],
        up_weight[0],
        down_weight[0],
        expert_total,
    )[None]


def solution(mesh):
    return jax.shard_map(
        per_device,
        mesh=mesh,
        in_specs=(
            P("dp", "sp", None),
            P("dp", "sp", None),
            P("dp", "sp", None),
            P("dp", "sp", None),
            P(),
            P(),
            P(),
            P(),
            P(),
            P(),
            P(),
            P(),
            P("dp", "sp", None),
            P("dp", "sp"),
            P("dp", "sp", None),
            P(("sp", "dp"), None, None),
            P(("sp", "dp"), None, None),
            P(("sp", "dp"), None, None),
        ),
        out_specs=P("dp", "sp", None),
        check_vma=False,
    )
```

```python
import functools

import jax
import jax.numpy as jnp
import numpy as np
from jax import lax
from jax.experimental import pallas as pl
from jax.experimental.pallas import tpu as pltpu
from jax.sharding import PartitionSpec as P

GROUPS = 4
SPAN = 64


eps = 1e-06


def dot32(a, b):
    return jnp.dot(a, b, preferred_element_type=jnp.float32)


def dot_t(a, b):
    return lax.dot_general(a, b, (((0,), (0,)), ((), ())), preferred_element_type=jnp.float32)


def layer_kernel(
    n_sp,
    n_y,
    n_dp,
    nope,
    rope,
    value_width,
    cap,
    top,
    residual_hbm,
    query_hbm,
    latent_hbm,
    rope_t_hbm,
    latent_gain_hbm,
    query_gain_hbm,
    key_gain_hbm,
    key_weight_hbm,
    value_weight_hbm,
    mix_gain_hbm,
    out_weight_hbm,
    ffn_gain_hbm,
    choice_hbm,
    group_prob_hbm,
    share_hbm,
    gate_hbm,
    up_hbm,
    down_hbm,
    near_hbm,
    far_hbm,
    out_ref,
    residual_ref,
    latent_ref,
    rope_t_ref,
    latent_gain_ref,
    query_gain_ref,
    key_gain_ref,
    key_weight_ref,
    value_weight_ref,
    mix_gain_ref,
    out_weight_ref,
    ffn_gain_ref,
    choice_ref,
    group_prob_ref,
    share_ref,
    gate_ref,
    up_ref,
    down_ref,
    near_ref,
    far_ref,
    wide_key,
    pick_query,
    turn_query,
    queries_in,
    packed,
    packed_in,
    queries,
    keys,
    values,
    bias,
    weights,
    heads_out,
    token_in,
    normed_ref,
    info_ref,
    pick_ref,
    out1,
    in1,
    out2,
    arrive,
    served,
    back2,
    merged,
    home,
    acc,
    w_sem,
    sq,
    rq,
    sz,
    rz,
    sy,
    ry,
    so,
    ro,
    s1,
    r1,
    s2,
    r2,
    s3,
    r3,
    s4,
    r4,
):
    bf = jnp.bfloat16
    f32 = jnp.float32
    tok = latent_ref.shape[0]
    width = out_ref.shape[1]
    qk = nope + rope
    half = rope // 2
    n_z = n_sp // n_y
    heads = n_z
    slot = 128
    wide_q = heads * qk
    wide_v = heads * value_width
    me = lax.axis_index("sp")
    z = me // n_y
    y = me % n_y

    def query_part(target):
        return query_hbm.at[:, pl.ds(pl.multiple_of(target * wide_q, slot), wide_q)]

    own_part = pl.ds(pl.multiple_of(z * wide_v, slot), wide_v)
    pairs = [
        (latent_hbm, latent_ref),
        (latent_gain_hbm, latent_gain_ref),
        (rope_t_hbm, rope_t_ref),
        (key_weight_hbm.at[:, own_part], key_weight_ref),
        (value_weight_hbm.at[:, own_part], value_weight_ref),
        (near_hbm, near_ref),
        (far_hbm, far_ref),
        (query_gain_hbm, query_gain_ref),
        (key_gain_hbm, key_gain_ref),
        (query_part(z), queries_in.at[z]),
        (choice_hbm, choice_ref),
        (group_prob_hbm, group_prob_ref),
        (share_hbm, share_ref),
        (mix_gain_hbm, mix_gain_ref),
        (ffn_gain_hbm, ffn_gain_ref),
        (residual_hbm, residual_ref),
        (out_weight_hbm, out_weight_ref),
        (gate_hbm, gate_ref),
        (up_hbm, up_ref),
        (down_hbm, down_ref),
    ]
    loads = [
        pltpu.make_async_copy(src, dst, w_sem.at[n]) for n, (src, dst) in enumerate(pairs)
    ]
    small = 15
    for load in loads[:small]:
        load.start()

    def remote(src, dst, send, recv, target):
        return pltpu.make_async_remote_copy(
            src_ref=src,
            dst_ref=dst,
            send_sem=send,
            recv_sem=recv,
            device_id=target if isinstance(target, dict) else {"sp": target},
            device_id_type=pl.DeviceIdType.MESH,
        )

    dp = lax.axis_index("dp")
    peers = n_y * n_dp
    rows = tok // top
    mine = y * n_dp + dp

    def peer(j):
        other = (mine + j) % peers
        return {"sp": z * n_y + other // n_dp, "dp": other % n_dp}

    def at_z(k):
        return ((z + k) % n_z) * n_y + y

    def at_y(m):
        return z * n_y + (y + m) % n_y

    barrier = pltpu.get_barrier_semaphore()
    for target in [{"sp": at_z(k)} for k in range(1, n_z)] + [peer(j) for j in range(1, peers)]:
        pl.semaphore_signal(
            barrier, inc=1, device_id=target, device_id_type=pl.DeviceIdType.MESH
        )
    for load in loads[:3]:
        load.wait()
    raw = latent_ref[...].astype(f32)
    scale = lax.rsqrt(jnp.mean(raw * raw, axis=-1, keepdims=True) + eps)
    packed[:tok] = (raw * scale * latent_gain_ref[...]).astype(bf)
    packed[tok:, :tok] = rope_t_ref[:half]
    packed[tok:, tok:] = rope_t_ref[half:]
    pl.semaphore_wait(barrier, n_z - 1 + peers - 1)

    sent = []
    down = {}
    for k in (1, 3, 2):
        down[k] = remote(packed, packed_in.at[me], sz.at[k], rz.at[k], at_z(k))
        down[k].start()

    def spread(k, source):
        index = ((z + n_z - k) % n_z) * n_y + y
        for m in (1, 3, 2):
            sent.append(remote(source, packed_in.at[index], sy.at[k, m], ry.at[k, m], at_y(m)))
            sent[-1].start()

    spread(0, packed)
    asked = []
    for k in (1, 3, 2):
        target = (z + k) % n_z
        asked.append(remote(query_part(target), queries_in.at[z], sq.at[k], rq.at[k], at_z(k)))
        asked[-1].start()

    for load in loads[small:]:
        load.start()
    packed_in[me] = packed[...]

    def selector(rows, columns, source):
        i = lax.broadcasted_iota(jnp.int32, (rows, columns), 0)
        c = lax.broadcasted_iota(jnp.int32, (rows, columns), 1)
        return (i == source(c // slot, c % slot)).astype(f32).astype(bf)

    def swapped(c):
        return jnp.where(
            c < nope, -1, jnp.where(c < nope + half, c + half, jnp.where(c < qk, c - half, -1))
        )

    def plain_of(c, first):
        return jnp.where((c >= first) & (c < qk), c, -1)

    def route():
        lower = lax.broadcasted_iota(jnp.int32, (tok, tok), 0)
        upper = lax.broadcasted_iota(jnp.int32, (tok, tok), 1)
        before = (lower < upper).astype(f32).astype(bf)
        per_group = peers
        chosen = choice_ref[...]
        group = chosen[0:1] // per_group
        of_group = (
            lax.broadcasted_iota(jnp.int32, (8, tok), 0) == jnp.broadcast_to(group, (8, tok))
        ).astype(f32)
        rank = jnp.sum(of_group * dot32(of_group.astype(bf), before), axis=0, keepdims=True)
        line = group * rows + rank.astype(jnp.int32)
        place = lax.broadcasted_iota(jnp.int32, (n_z * rows, tok), 0)
        pick = (place == jnp.broadcast_to(line, place.shape)).astype(f32).astype(bf)
        for g in range(n_z):
            pick_ref[g] = pick[g * rows : (g + 1) * rows]
        expert = lax.broadcasted_iota(jnp.int32, (n_z * per_group, tok), 0)
        of_expert = [
            (expert == jnp.broadcast_to(chosen[t : t + 1], expert.shape)).astype(f32)
            for t in range(top)
        ]
        named = of_expert[0]
        for t in range(1, top):
            named = named + of_expert[t]
        count = dot32(named.astype(bf), before)
        share = share_ref[...]
        whole = share[0:1]
        for t in range(1, top):
            whole = whole + share[t : t + 1]
        lines = []
        for t in range(top):
            earlier = jnp.sum(of_expert[t] * count, axis=0, keepdims=True)
            local_one = ((chosen[t : t + 1] - group * per_group) * cap).astype(f32)
            lines.append(local_one + earlier)
        for t in range(top):
            part = group_prob_ref[...] * share[t : t + 1] / whole
            high = part.astype(bf).astype(f32)
            lines += [high, part - high]
        at = lax.broadcasted_iota(jnp.int32, (slot, tok), 0)
        total = jnp.zeros((slot, tok), f32)
        for n, values_of in enumerate(lines):
            total = jnp.where(at == n, jnp.broadcast_to(values_of, at.shape), total)
        info_ref[...] = total.astype(bf)

    pick_query[...] = selector(
        wide_q, heads * slot, lambda h, c: jnp.where(c < qk, c + h * qk, -1)
    )
    turn_query[...] = selector(
        wide_q,
        heads * slot,
        lambda h, c: jnp.where((c >= nope) & (c < qk), swapped(c) + h * qk, -1),
    )
    pick_rope = selector(
        rope,
        2 * slot,
        lambda h, c: jnp.where(
            (c < nope) | (c >= qk), -1, jnp.where(h == 0, c, swapped(c)) - nope
        ),
    )
    q_pos = y * tok + lax.broadcasted_iota(jnp.int32, bias.shape, 0)
    k_pos = lax.broadcasted_iota(jnp.int32, bias.shape, 1)
    bias[...] = jnp.where(k_pos // SPAN <= q_pos // SPAN, 0.0, -1e30)
    loads[3].wait()
    wide_key[...] = dot32(
        key_weight_ref[...],
        selector(heads * nope, heads * slot, lambda h, c: jnp.where(c < nope, c + h * nope, -1)),
    ).astype(bf)
    for load in loads[4:small]:
        load.wait()
    route()

    for k in (1, 3, 2):
        down[k].wait_recv()
        spread(k, packed_in.at[((z + n_z - k) % n_z) * n_y + y])

    near_cos, near_sin = near_ref[0], near_ref[1]

    def tables(block):
        far_cos = far_ref[0, pl.ds(block, 1), :]
        far_sin = far_ref[1, pl.ds(block, 1), :]
        return (
            far_cos * near_cos - far_sin * near_sin,
            far_sin * near_cos + far_cos * near_sin,
        )

    def both(gain_ref):
        gain = jnp.concatenate([gain_ref[...], jnp.zeros((1, slot - qk), f32)], axis=1)
        gain = jnp.broadcast_to(gain, (8, slot))
        c = lax.broadcasted_iota(jnp.int32, (8, slot), 1)
        up = pltpu.roll(gain, half, 1)
        down_by = pltpu.roll(gain, slot - half, 1)
        turned = jnp.where(
            c < nope, 0.0, jnp.where(c < nope + half, -down_by, jnp.where(c < qk, up, 0.0))
        )
        return gain[0:1], turned[0:1]

    query_gain, query_swap = both(query_gain_ref)
    key_gain, key_swap = both(key_gain_ref)

    def prepare(i, carry):
        step = i // n_y
        k = jnp.where(step < 2, step, 5 - step)
        m = i % n_y
        origin = (z + n_z - k) % n_z
        s = origin * n_y + (y + n_y - m) % n_y

        @pl.when(m > 0)
        def _():
            remote(packed, packed_in.at[s], sy.at[k, m], ry.at[k, m], me).wait_recv()

        at = pl.ds(pl.multiple_of(s * tok, tok), tok)
        block = packed_in[s]
        latent = block[:tok]
        values[at, :] = dot32(latent, value_weight_ref[...]).astype(bf)
        part = dot32(latent, wide_key[...]).astype(bf).astype(f32)
        turned_rows = jnp.concatenate([block[tok:, :tok], block[tok:, tok:]], axis=0)
        spun = dot_t(turned_rows, pick_rope)
        cos, sin = tables(s)
        plain_rope = spun[:, :slot]
        tail = plain_rope * (key_gain * cos) + spun[:, slot:] * (key_swap * sin)
        for h in range(heads):
            own = part[:, h * slot : (h + 1) * slot]
            full = own + plain_rope
            norm = lax.rsqrt(jnp.sum(full * full, axis=-1, keepdims=True) / qk + eps)
            keys[h, at, :] = ((own * key_gain + tail) * norm).astype(bf)
        return carry

    lax.fori_loop(0, n_sp, prepare, 0)

    for copy in asked:
        copy.wait_recv()

    def prepare_queries(b, carry):
        raw = queries_in[b]
        plain = dot32(raw, pick_query[...])
        turned = dot32(raw, turn_query[...])
        cos, sin = tables(b * n_y + y)
        for h in range(heads):
            span = slice(h * slot, (h + 1) * slot)
            own = plain[:, span]
            norm = lax.rsqrt(jnp.sum(own * own, axis=-1, keepdims=True) / qk + eps)
            queries[b, h] = (
                (own * (query_gain * cos) + turned[:, span] * (query_swap * sin)) * norm
            ).astype(bf)
        return carry

    lax.fori_loop(0, n_z, prepare_queries, 0)

    stretch = n_y * tok
    factor = qk ** (-0.5) * 1.4426950408889634
    lane = lax.broadcasted_iota(jnp.int32, (tok, wide_v), 1) // value_width
    for b in range(n_z - 1, -1, -1):
        last = (b + 1) * stretch
        sums = []
        for h in range(heads):
            scores = lax.dot_general(
                queries[b, h],
                keys[h, :last],
                (((1,), (1,)), ((), ())),
                preferred_element_type=f32,
            )
            edge = scores[:, last - stretch :] + bias[...]
            top = jnp.max(edge, axis=-1, keepdims=True)
            if b:
                inner = scores[:, : last - stretch]
                top = jnp.maximum(top, jnp.max(inner, axis=-1, keepdims=True))
            raised = jnp.exp2((edge - top) * factor)
            total = jnp.sum(raised, axis=-1, keepdims=True)
            weights[h * tok : (h + 1) * tok, last - stretch : last] = raised.astype(bf)
            if b:
                raised = jnp.exp2((inner - top) * factor)
                total = total + jnp.sum(raised, axis=-1, keepdims=True)
                weights[h * tok : (h + 1) * tok, : last - stretch] = raised.astype(bf)
            sums.append(total)
        mixed = dot32(weights[:, :last], values[:last])
        total = None
        for h in range(heads):
            own = mixed[h * tok : (h + 1) * tok] / sums[h]
            total = own if total is None else jnp.where(lane < h, total, own)
        heads_out[b] = total.astype(bf)

        @pl.when(z != b)
        def _():
            remote(
                heads_out.at[b], token_in.at[z], so.at[b], ro.at[z], b * n_y + y
            ).start()

    token_in[z] = heads_out[z]
    for load in loads[small:]:
        load.wait()
    for k in range(1, n_z):
        other = (z + k) % n_z
        remote(
            heads_out.at[other], token_in.at[other], so.at[other], ro.at[other], other * n_y + y
        ).wait()
    square = None
    for s in range(n_z):
        piece = token_in[s].astype(f32)
        part = jnp.sum(piece * piece, axis=-1, keepdims=True)
        square = part if square is None else square + part
    scale = lax.rsqrt(square / (n_z * wide_v) + eps)
    mixed = jnp.concatenate(
        [
            (token_in[s].astype(f32) * scale * mix_gain_ref[:, s * wide_v : (s + 1) * wide_v]).astype(bf)
            for s in range(n_z)
        ],
        axis=1,
    )
    stream = residual_ref[...].astype(f32) + dot32(mixed, out_weight_ref[...])
    acc[...] = stream
    scale = lax.rsqrt(jnp.mean(stream * stream, axis=-1, keepdims=True) + eps)
    normed_ref[...] = (stream * scale * ffn_gain_ref[...]).astype(bf)

    first = {}

    def pack(k, target):
        picks = pick_ref[(z + k) % n_z]
        target[k, :, :width] = dot32(picks, normed_ref[...]).astype(bf)
        target[k, :, width:] = lax.dot_general(
            picks, info_ref[...], (((1,), (1,)), ((), ())), preferred_element_type=f32
        ).astype(bf)

    for k in (1, 3, 2):
        pack(k, out1)
        first[k] = remote(out1.at[k], in1.at[k], s1.at[k], r1.at[k], at_z(k))
        first[k].start()
    pack(0, in1)

    def slots(k):
        info = in1[k, :, width:].astype(f32)
        place = lax.broadcasted_iota(jnp.int32, (rows, peers * cap), 1).astype(f32)
        return place == info[:, 0:1], place == info[:, 1:2], info

    second = {}

    def scatter(k):
        if k:
            first[k].wait_recv()
        at0, at1, _ = slots(k)
        choose = (at0.astype(f32) + at1.astype(f32)).astype(bf)
        placed = dot_t(choose, in1[k, :, :width]).astype(bf)
        for e in range(peers):
            out2[k, e] = placed[e * cap : (e + 1) * cap]
        second[k] = [
            remote(
                out2.at[k, (mine + j) % peers], arrive.at[k, j], s2.at[k, j], r2.at[k, j], peer(j)
            )
            for j in range(1, peers)
        ]
        for copy in second[k]:
            copy.start()
        arrive[k, 0] = out2[k, mine]

    third = {}

    def serve(k):
        for copy in second[k]:
            copy.wait_recv()
        given = arrive[k].reshape(peers * cap, width)
        gate_act = dot32(given, gate_ref[...])
        upward = dot32(given, up_ref[...])
        hidden = (gate_act * (1.0 / (1.0 + jnp.exp(-gate_act))) * upward).astype(bf)
        result = dot32(hidden, down_ref[...]).astype(bf)
        for j in range(peers):
            served[k, j] = result[j * cap : (j + 1) * cap]
        third[k] = [
            remote(
                served.at[k, j], back2.at[k, mine], s3.at[k, j], r3.at[k, peers - j], peer(peers - j)
            )
            for j in range(1, peers)
        ]
        for copy in third[k]:
            copy.start()
        back2[k, mine] = served[k, 0]

    fourth = {}

    def merge(k):
        for copy in third[k]:
            copy.wait_recv()
        at0, at1, info = slots(k)
        high = jnp.where(at0, info[:, 2:3], 0.0) + jnp.where(at1, info[:, 4:5], 0.0)
        low = jnp.where(at0, info[:, 3:4], 0.0) + jnp.where(at1, info[:, 5:6], 0.0)
        got = back2[k].reshape(peers * cap, width)
        total = dot32(high.astype(bf), got) + dot32(low.astype(bf), got)
        if k:
            merged[k] = total.astype(bf)
            fourth[k] = remote(merged.at[k], home.at[k], s4.at[k], r4.at[k], at_z(n_z - k))
            fourth[k].start()
        else:
            acc[...] += dot_t(pick_ref[z], total.astype(bf))

    for k in (0, 1, 3, 2):
        scatter(k)
    for k in (1, 3, 2, 0):
        serve(k)
    for k in (1, 3, 2, 0):
        merge(k)
    for k in (1, 3, 2):
        fourth[k].wait_recv()
        acc[...] += dot_t(pick_ref[(z + k) % n_z], home[k])
    out_ref[...] = acc[...].astype(bf)
    for copy in list(down.values()) + sent + asked:
        copy.wait_send()
    for k in range(n_z):
        if k:
            first[k].wait_send()
            fourth[k].wait_send()
        for copy in second[k] + third[k]:
            copy.wait_send()


def trig(positions, nope, rope):
    frequency = 10000.0 ** (-2.0 * np.arange(rope // 2) / rope)
    angle = np.asarray(positions, np.float64)[:, None] * frequency[None, :]
    cos = np.ones((len(positions), 128))
    sin = np.zeros((len(positions), 128))
    cos[:, nope : nope + rope] = np.concatenate([np.cos(angle)] * 2, axis=1)
    sin[:, nope : nope + rope] = np.concatenate([np.sin(angle)] * 2, axis=1)
    return np.stack([cos, sin]).astype(np.float32)


def per_device(
    residual,
    query,
    latent,
    rope_key,
    latent_gain,
    query_gain,
    key_gain,
    key_weight,
    value_weight,
    mix_gain,
    out_weight,
    ffn_gain,
    expert_choice,
    group_prob,
    expert_prob,
    gate_weight,
    up_weight,
    down_weight,
):
    n_sp = lax.axis_size("sp")
    n_dp = lax.axis_size("dp")
    n_z = GROUPS
    n_y = n_sp // n_z
    tok, width = residual.shape[1:]
    rope = rope_key.shape[2]
    qk = query_gain.shape[0]
    nope = qk - rope
    lat = latent.shape[2]
    head_count = query.shape[2] // qk
    value_width = value_weight.shape[1] // head_count
    heads = head_count // n_z
    length = n_sp * tok
    half = rope // 2
    top = expert_choice.shape[2]
    peers = n_y * n_dp
    cap = tok // peers
    rows = tok // top
    hidden = gate_weight.shape[2]
    slot = 128
    wide_v = heads * value_width
    bf = jnp.bfloat16
    f32 = jnp.float32
    near = jnp.asarray(trig(np.arange(tok), nope, rope))
    far = jnp.asarray(trig(np.arange(n_sp) * tok, nope, rope))
    vmem = pltpu.VMEM
    hbm = pl.BlockSpec(memory_space=pl.ANY)
    dma = pltpu.SemaphoreType.DMA
    out = pl.pallas_call(
        functools.partial(
            layer_kernel, n_sp, n_y, n_dp, nope, rope, value_width, cap, top
        ),
        out_shape=jax.ShapeDtypeStruct((tok, width), bf),
        in_specs=[hbm] * 20,
        out_specs=pl.BlockSpec(memory_space=vmem),
        scratch_shapes=[
            vmem((tok, width), bf),
            vmem((tok, lat), bf),
            vmem((rope, tok), bf),
            vmem((1, lat), f32),
            vmem((1, qk), f32),
            vmem((1, qk), f32),
            vmem((lat, wide_v), bf),
            vmem((lat, wide_v), bf),
            vmem((1, head_count * value_width), f32),
            vmem(out_weight.shape, bf),
            vmem((1, width), f32),
            vmem((top, tok), jnp.int32),
            vmem((1, tok), f32),
            vmem((top, tok), f32),
            vmem((width, hidden), bf),
            vmem((width, hidden), bf),
            vmem((hidden, width), bf),
            vmem(near.shape, f32),
            vmem(far.shape, f32),
            vmem((lat, heads * slot), bf),
            vmem((heads * qk, heads * slot), bf),
            vmem((heads * qk, heads * slot), bf),
            vmem((n_z, tok, heads * qk), bf),
            vmem((tok + half, lat), bf),
            vmem((n_sp, tok + half, lat), bf),
            vmem((n_z, heads, tok, slot), bf),
            vmem((heads, length, slot), bf),
            vmem((length, wide_v), bf),
            vmem((tok, n_y * tok), f32),
            vmem((heads * tok, length), bf),
            vmem((n_z, tok, wide_v), bf),
            vmem((n_z, tok, wide_v), bf),
            vmem((tok, width), bf),
            vmem((slot, tok), bf),
            vmem((n_z, rows, tok), bf),
            vmem((n_z, rows, width + slot), bf),
            vmem((n_z, rows, width + slot), bf),
            vmem((n_z, peers, cap, width), bf),
            vmem((n_z, peers, cap, width), bf),
            vmem((n_z, peers, cap, width), bf),
            vmem((n_z, peers, cap, width), bf),
            vmem((n_z, rows, width), bf),
            vmem((n_z, rows, width), bf),
            vmem((tok, width), f32),
            dma((20,)),
            dma((n_z,)),
            dma((n_z,)),
            dma((n_z,)),
            dma((n_z,)),
            dma((n_z, n_y)),
            dma((n_z, n_y)),
            dma((n_z,)),
            dma((n_z,)),
            dma((n_z,)),
            dma((n_z,)),
            dma((n_z, peers)),
            dma((n_z, peers)),
            dma((n_z, peers)),
            dma((n_z, peers)),
            dma((n_z,)),
            dma((n_z,)),
        ],
        compiler_params=pltpu.CompilerParams(
            collective_id=0, has_side_effects=True, vmem_limit_bytes=67043328
        ),
    )(
        residual[0],
        query[0],
        latent[0],
        rope_key[0].T,
        latent_gain[None],
        query_gain[None],
        key_gain[None],
        key_weight,
        value_weight,
        mix_gain[None],
        out_weight,
        ffn_gain[None],
        expert_choice[0].T,
        group_prob,
        expert_prob[0].T,
        gate_weight[0],
        up_weight[0],
        down_weight[0],
        near,
        far,
    )
    return out[None]


def solution(mesh):
    return jax.shard_map(
        per_device,
        mesh=mesh,
        in_specs=(
            P("dp", "sp", None),
            P("dp", "sp", None),
            P("dp", "sp", None),
            P("dp", "sp", None),
            P(),
            P(),
            P(),
            P(),
            P(),
            P(),
            P(),
            P(),
            P("dp", "sp", None),
            P("dp", "sp"),
            P("dp", "sp", None),
            P(("sp", "dp"), None, None),
            P(("sp", "dp"), None, None),
            P(("sp", "dp"), None, None),
        ),
        out_specs=P("dp", "sp", None),
        check_vma=False,
    )
```

```python
import functools

import jax
import jax.numpy as jnp
import numpy as np
from jax import lax
from jax.experimental import pallas as pl
from jax.experimental.pallas import tpu as pltpu
from jax.sharding import PartitionSpec as P

GROUPS = 4
SPAN = 64


eps = 1e-06


def dot32(a, b):
    return jnp.dot(a, b, preferred_element_type=jnp.float32)


def dot_t(a, b):
    return lax.dot_general(a, b, (((0,), (0,)), ((), ())), preferred_element_type=jnp.float32)


def layer_kernel(
    n_sp,
    n_y,
    n_dp,
    nope,
    rope,
    value_width,
    cap,
    top,
    residual_hbm,
    query_hbm,
    latent_hbm,
    rope_t_hbm,
    latent_gain_hbm,
    query_gain_hbm,
    key_gain_hbm,
    key_weight_hbm,
    value_weight_hbm,
    mix_gain_hbm,
    out_weight_hbm,
    ffn_gain_hbm,
    choice_hbm,
    group_prob_hbm,
    share_hbm,
    gate_hbm,
    up_hbm,
    down_hbm,
    near_hbm,
    far_hbm,
    pick_query_hbm,
    spread_key_hbm,
    pick_rope_hbm,
    out_ref,
    residual_ref,
    latent_ref,
    rope_t_ref,
    latent_gain_ref,
    query_gain_ref,
    key_gain_ref,
    key_weight_ref,
    value_weight_ref,
    mix_gain_ref,
    out_weight_ref,
    ffn_gain_ref,
    choice_ref,
    group_prob_ref,
    share_ref,
    gate_ref,
    up_ref,
    down_ref,
    near_ref,
    far_ref,
    wide_key,
    pick_query,
    spread_key,
    pick_rope,
    queries_in,
    packed,
    packed_in,
    queries,
    keys,
    values,
    bias,
    weights,
    heads_out,
    token_in,
    normed_ref,
    info_ref,
    pick_ref,
    out1,
    in1,
    out2,
    arrive,
    served,
    back2,
    merged,
    home,
    acc,
    w_sem,
    sq,
    rq,
    sz,
    rz,
    sv,
    rv,
    sy,
    ry,
    sx,
    rx,
    so,
    ro,
    s1,
    r1,
    s2,
    r2,
    s3,
    r3,
    s4,
    r4,
):
    bf = jnp.bfloat16
    f32 = jnp.float32
    tok = latent_ref.shape[0]
    width = out_ref.shape[1]
    qk = nope + rope
    half = rope // 2
    n_z = n_sp // n_y
    heads = n_z
    slot = 128
    wide_q = heads * qk
    wide_v = heads * value_width
    me = lax.axis_index("sp")
    z = me // n_y
    y = me % n_y

    def query_part(target):
        return query_hbm.at[:, pl.ds(pl.multiple_of(target * wide_q, slot), wide_q)]

    own_part = pl.ds(pl.multiple_of(z * wide_v, slot), wide_v)
    pairs = [
        (latent_hbm, latent_ref),
        (latent_gain_hbm, latent_gain_ref),
        (rope_t_hbm, rope_t_ref),
        (key_weight_hbm.at[:, own_part], key_weight_ref),
        (value_weight_hbm.at[:, own_part], value_weight_ref),
        (near_hbm, near_ref),
        (pick_rope_hbm, pick_rope),
        (spread_key_hbm, spread_key),
        (pick_query_hbm, pick_query),
        (far_hbm, far_ref),
        (query_gain_hbm, query_gain_ref),
        (key_gain_hbm, key_gain_ref),
        (query_part(z), queries_in.at[z]),
        (choice_hbm, choice_ref),
        (group_prob_hbm, group_prob_ref),
        (share_hbm, share_ref),
        (mix_gain_hbm, mix_gain_ref),
        (ffn_gain_hbm, ffn_gain_ref),
        (residual_hbm, residual_ref),
        (out_weight_hbm, out_weight_ref),
        (gate_hbm, gate_ref),
        (up_hbm, up_ref),
        (down_hbm, down_ref),
    ]
    loads = [
        pltpu.make_async_copy(src, dst, w_sem.at[n]) for n, (src, dst) in enumerate(pairs)
    ]
    small = 18
    for load in loads[:small]:
        load.start()

    def remote(src, dst, send, recv, target):
        return pltpu.make_async_remote_copy(
            src_ref=src,
            dst_ref=dst,
            send_sem=send,
            recv_sem=recv,
            device_id=target if isinstance(target, dict) else {"sp": target},
            device_id_type=pl.DeviceIdType.MESH,
        )

    dp = lax.axis_index("dp")
    peers = n_y * n_dp
    rows = tok // top
    mine = y * n_dp + dp

    def peer(j):
        other = (mine + j) % peers
        return {"sp": z * n_y + other // n_dp, "dp": other % n_dp}

    def at_z(k):
        return ((z + k) % n_z) * n_y + y

    def at_y(m):
        return z * n_y + (y + m) % n_y

    barrier = pltpu.get_barrier_semaphore()
    greeted = [{"sp": at_z(k)} for k in range(1, n_z)] + [{"sp": at_y(m)} for m in range(1, n_y)]
    greeted += [{"dp": (dp + d) % n_dp} for d in range(1, n_dp)]
    for target in greeted:
        pl.semaphore_signal(
            barrier, inc=1, device_id=target, device_id_type=pl.DeviceIdType.MESH
        )
    for load in loads[:3]:
        load.wait()
    raw = latent_ref[...].astype(f32)
    scale = lax.rsqrt(jnp.mean(raw * raw, axis=-1, keepdims=True) + eps)
    packed[:tok] = (raw * scale * latent_gain_ref[...]).astype(bf)
    packed[tok:, :tok] = rope_t_ref[:half]
    packed[tok:, tok:] = rope_t_ref[half:]
    pl.semaphore_wait(barrier, len(greeted))

    sent = []
    asked = []
    down = {}
    over = {}
    cut = packed.shape[0] * 5 // 9

    def spread_y(k, source):
        origin = at_z(n_z - k) if k else me
        for m in (1, 3, 2):
            copy = remote(
                source, packed_in.at[origin, :cut], sy.at[k, m], ry.at[k, m], at_y(m)
            )
            copy.start()
            sent.append(copy)

    def spread_z(m, source):
        origin = at_y(n_y - m) if m else me
        for k in (1, 3, 2):
            copy = remote(
                source, packed_in.at[origin, cut:], sx.at[m, k], rx.at[m, k], at_z(k)
            )
            copy.start()
            sent.append(copy)

    def ask():
        for k in (1, 3, 2):
            target = (z + k) % n_z
            copy = remote(query_part(target), queries_in.at[z], sq.at[k], rq.at[k], at_z(k))
            copy.start()
            asked.append(copy)

    for k in (1, 3, 2):
        down[k] = remote(
            packed.at[:cut], packed_in.at[me, :cut], sz.at[k], rz.at[k], at_z(k)
        )
        down[k].start()
        over[k] = remote(
            packed.at[cut:], packed_in.at[me, cut:], sv.at[k], rv.at[k], at_y(k)
        )
        over[k].start()
    spread_y(0, packed.at[:cut])
    spread_z(0, packed.at[cut:])
    packed_in[me] = packed[...]

    def route():
        lower = lax.broadcasted_iota(jnp.int32, (tok, tok), 0)
        upper = lax.broadcasted_iota(jnp.int32, (tok, tok), 1)
        before = (lower < upper).astype(f32).astype(bf)
        per_group = peers
        chosen = choice_ref[...]
        group = chosen[0:1] // per_group
        of_group = (
            lax.broadcasted_iota(jnp.int32, (8, tok), 0) == jnp.broadcast_to(group, (8, tok))
        ).astype(f32)
        rank = jnp.sum(of_group * dot32(of_group.astype(bf), before), axis=0, keepdims=True)
        line = group * rows + rank.astype(jnp.int32)
        place = lax.broadcasted_iota(jnp.int32, (n_z * rows, tok), 0)
        pick = (place == jnp.broadcast_to(line, place.shape)).astype(f32).astype(bf)
        for g in range(n_z):
            pick_ref[g] = pick[g * rows : (g + 1) * rows]
        expert = lax.broadcasted_iota(jnp.int32, (n_z * per_group, tok), 0)
        of_expert = [
            (expert == jnp.broadcast_to(chosen[t : t + 1], expert.shape)).astype(f32)
            for t in range(top)
        ]
        named = of_expert[0]
        for t in range(1, top):
            named = named + of_expert[t]
        count = dot32(named.astype(bf), before)
        share = share_ref[...]
        whole = share[0:1]
        for t in range(1, top):
            whole = whole + share[t : t + 1]
        lines = []
        for t in range(top):
            earlier = jnp.sum(of_expert[t] * count, axis=0, keepdims=True)
            local_one = ((chosen[t : t + 1] - group * per_group) * cap).astype(f32)
            lines.append(local_one + earlier)
        for t in range(top):
            part = group_prob_ref[...] * share[t : t + 1] / whole
            high = part.astype(bf).astype(f32)
            lines += [high, part - high]
        at = lax.broadcasted_iota(jnp.int32, (slot, tok), 0)
        total = jnp.zeros((slot, tok), f32)
        for n, values_of in enumerate(lines):
            total = jnp.where(at == n, jnp.broadcast_to(values_of, at.shape), total)
        info_ref[...] = total.astype(bf)

    gaps = [(1, 1), (3, 3), (2, 2)]
    for k, m in gaps:
        down[k].wait_recv()
        spread_y(k, packed_in.at[at_z(n_z - k), :cut])
        over[m].wait_recv()
        spread_z(m, packed_in.at[at_y(n_y - m), cut:])
    ask()

    for load in loads[small:]:
        load.start()
    for load in loads[3:small]:
        load.wait()
    q_pos = y * tok + lax.broadcasted_iota(jnp.int32, bias.shape, 0)
    k_pos = lax.broadcasted_iota(jnp.int32, bias.shape, 1)
    bias[...] = jnp.where(k_pos // SPAN <= q_pos // SPAN, 0.0, -1e30)
    wide_key[...] = dot32(key_weight_ref[...], spread_key[...]).astype(bf)
    route()

    near_cos, near_sin = near_ref[0], near_ref[1]

    def tables(block):
        far_cos = far_ref[0, pl.ds(block, 1), :]
        far_sin = far_ref[1, pl.ds(block, 1), :]
        return (
            far_cos * near_cos - far_sin * near_sin,
            far_sin * near_cos + far_cos * near_sin,
        )

    def both(gain_ref):
        gain = jnp.concatenate([gain_ref[...], jnp.zeros((1, slot - qk), f32)], axis=1)
        gain = jnp.broadcast_to(gain, (8, slot))
        c = lax.broadcasted_iota(jnp.int32, (8, slot), 1)
        up = pltpu.roll(gain, half, 1)
        down_by = pltpu.roll(gain, slot - half, 1)
        turned = jnp.where(
            c < nope, 0.0, jnp.where(c < nope + half, -down_by, jnp.where(c < qk, up, 0.0))
        )
        return gain[0:1], turned[0:1]

    query_gain, query_swap = both(query_gain_ref)
    key_gain, key_swap = both(key_gain_ref)

    def prepare(i, carry):
        step = i // n_y
        k = jnp.where(step < 2, step, 5 - step)
        m = i % n_y
        origin = (z + n_z - k) % n_z
        s = origin * n_y + (y + n_y - m) % n_y

        @pl.when(m > 0)
        def _():
            part = packed_in.at[s, :cut]
            remote(part, part, sy.at[k, m], ry.at[k, m], me).wait_recv()

        @pl.when(k > 0)
        def _():
            part = packed_in.at[s, cut:]
            remote(part, part, sx.at[m, k], rx.at[m, k], me).wait_recv()

        at = pl.ds(pl.multiple_of(s * tok, tok), tok)
        block = packed_in[s]
        latent = block[:tok]
        values[at, :] = dot32(latent, value_weight_ref[...]).astype(bf)
        part = dot32(latent, wide_key[...]).astype(bf).astype(f32)
        turned_rows = jnp.concatenate([block[tok:, :tok], block[tok:, tok:]], axis=0)
        spun = dot_t(turned_rows, pick_rope[...])
        cos, sin = tables(s)
        plain_rope = spun[:, :slot]
        tail = plain_rope * (key_gain * cos) + spun[:, slot:] * (key_swap * sin)
        for h in range(heads):
            own = part[:, h * slot : (h + 1) * slot]
            full = own + plain_rope
            norm = lax.rsqrt(jnp.sum(full * full, axis=-1, keepdims=True) / qk + eps)
            keys[h, at, :] = ((own * key_gain + tail) * norm).astype(bf)
        return carry

    lax.fori_loop(0, n_sp, prepare, 0)

    for copy in asked:
        copy.wait_recv()

    def prepare_queries(b, carry):
        raw = queries_in[b]
        both_parts = dot32(raw, pick_query[...])
        plain, turned = both_parts[:, : heads * slot], both_parts[:, heads * slot :]
        cos, sin = tables(b * n_y + y)
        for h in range(heads):
            span = slice(h * slot, (h + 1) * slot)
            own = plain[:, span]
            norm = lax.rsqrt(jnp.sum(own * own, axis=-1, keepdims=True) / qk + eps)
            queries[b, h] = (
                (own * (query_gain * cos) + turned[:, span] * (query_swap * sin)) * norm
            ).astype(bf)
        return carry

    lax.fori_loop(0, n_z, prepare_queries, 0)

    stretch = n_y * tok
    factor = qk ** (-0.5) * 1.4426950408889634
    lane = lax.broadcasted_iota(jnp.int32, (tok, wide_v), 1) // value_width
    for b in range(n_z - 1, -1, -1):
        last = (b + 1) * stretch
        sums = []
        for h in range(heads):
            scores = lax.dot_general(
                queries[b, h],
                keys[h, :last],
                (((1,), (1,)), ((), ())),
                preferred_element_type=f32,
            )
            edge = scores[:, last - stretch :] + bias[...]
            top = jnp.max(edge, axis=-1, keepdims=True)
            if b:
                inner = scores[:, : last - stretch]
                top = jnp.maximum(top, jnp.max(inner, axis=-1, keepdims=True))
            raised = jnp.exp2((edge - top) * factor)
            total = jnp.sum(raised, axis=-1, keepdims=True)
            weights[h * tok : (h + 1) * tok, last - stretch : last] = raised.astype(bf)
            if b:
                raised = jnp.exp2((inner - top) * factor)
                total = total + jnp.sum(raised, axis=-1, keepdims=True)
                weights[h * tok : (h + 1) * tok, : last - stretch] = raised.astype(bf)
            sums.append(total)
        mixed = dot32(weights[:, :last], values[:last])
        total = None
        for h in range(heads):
            own = mixed[h * tok : (h + 1) * tok] / sums[h]
            total = own if total is None else jnp.where(lane < h, total, own)
        heads_out[b] = total.astype(bf)

        @pl.when(z != b)
        def _():
            remote(
                heads_out.at[b], token_in.at[z], so.at[b], ro.at[z], b * n_y + y
            ).start()

    token_in[z] = heads_out[z]
    for load in loads[small:]:
        load.wait()
    for k in range(1, n_z):
        other = (z + k) % n_z
        remote(
            heads_out.at[other], token_in.at[other], so.at[other], ro.at[other], other * n_y + y
        ).wait()
    square = None
    for s in range(n_z):
        piece = token_in[s].astype(f32)
        part = jnp.sum(piece * piece, axis=-1, keepdims=True)
        square = part if square is None else square + part
    scale = lax.rsqrt(square / (n_z * wide_v) + eps)
    mixed = jnp.concatenate(
        [
            (token_in[s].astype(f32) * scale * mix_gain_ref[:, s * wide_v : (s + 1) * wide_v]).astype(bf)
            for s in range(n_z)
        ],
        axis=1,
    )
    stream = residual_ref[...].astype(f32) + dot32(mixed, out_weight_ref[...])
    acc[...] = stream
    scale = lax.rsqrt(jnp.mean(stream * stream, axis=-1, keepdims=True) + eps)
    normed_ref[...] = (stream * scale * ffn_gain_ref[...]).astype(bf)

    first = {}

    def pack(k, target):
        picks = pick_ref[(z + k) % n_z]
        target[k, :, :width] = dot32(picks, normed_ref[...]).astype(bf)
        target[k, :, width:] = lax.dot_general(
            picks, info_ref[...], (((1,), (1,)), ((), ())), preferred_element_type=f32
        ).astype(bf)

    for k in (1, 3, 2):
        pack(k, out1)
        first[k] = remote(out1.at[k], in1.at[k], s1.at[k], r1.at[k], at_z(k))
        first[k].start()
    pack(0, in1)

    def slots(k):
        info = in1[k, :, width:].astype(f32)
        place = lax.broadcasted_iota(jnp.int32, (rows, peers * cap), 1).astype(f32)
        return place == info[:, 0:1], place == info[:, 1:2], info

    second = {}

    def scatter(k):
        if k:
            first[k].wait_recv()
        at0, at1, _ = slots(k)
        choose = (at0.astype(f32) + at1.astype(f32)).astype(bf)
        placed = dot_t(choose, in1[k, :, :width]).astype(bf)
        for e in range(peers):
            out2[k, e] = placed[e * cap : (e + 1) * cap]
        second[k] = [
            remote(
                out2.at[k, (mine + j) % peers], arrive.at[k, j], s2.at[k, j], r2.at[k, j], peer(j)
            )
            for j in range(1, peers)
        ]
        for copy in second[k]:
            copy.start()
        arrive[k, 0] = out2[k, mine]

    third = {}

    def serve(k):
        for copy in second[k]:
            copy.wait_recv()
        given = arrive[k].reshape(peers * cap, width)
        gate_act = dot32(given, gate_ref[...])
        upward = dot32(given, up_ref[...])
        hidden = (gate_act * (1.0 / (1.0 + jnp.exp(-gate_act))) * upward).astype(bf)
        result = dot32(hidden, down_ref[...]).astype(bf)
        for j in range(peers):
            served[k, j] = result[j * cap : (j + 1) * cap]
        third[k] = [
            remote(
                served.at[k, j], back2.at[k, mine], s3.at[k, j], r3.at[k, peers - j], peer(peers - j)
            )
            for j in range(1, peers)
        ]
        for copy in third[k]:
            copy.start()
        back2[k, mine] = served[k, 0]

    fourth = {}

    def merge(k):
        for copy in third[k]:
            copy.wait_recv()
        at0, at1, info = slots(k)
        high = jnp.where(at0, info[:, 2:3], 0.0) + jnp.where(at1, info[:, 4:5], 0.0)
        low = jnp.where(at0, info[:, 3:4], 0.0) + jnp.where(at1, info[:, 5:6], 0.0)
        got = back2[k].reshape(peers * cap, width)
        total = dot32(high.astype(bf), got) + dot32(low.astype(bf), got)
        if k:
            merged[k] = total.astype(bf)
            fourth[k] = remote(merged.at[k], home.at[k], s4.at[k], r4.at[k], at_z(n_z - k))
            fourth[k].start()
        else:
            acc[...] += dot_t(pick_ref[z], total.astype(bf))

    for k in (0, 1, 3, 2):
        scatter(k)
    for k in (1, 3, 2, 0):
        serve(k)
    for k in (1, 3, 2, 0):
        merge(k)
    for k in (1, 3, 2):
        fourth[k].wait_recv()
        acc[...] += dot_t(pick_ref[(z + k) % n_z], home[k])
    out_ref[...] = acc[...].astype(bf)
    for copy in list(down.values()) + list(over.values()) + sent + asked:
        copy.wait_send()
    for k in range(n_z):
        if k:
            first[k].wait_send()
            fourth[k].wait_send()
        for copy in second[k] + third[k]:
            copy.wait_send()


def selector(rows, columns, slot, source):
    head, lane = np.divmod(np.arange(columns), slot)
    origin = np.asarray([source(h, c) for h, c in zip(head, lane)])
    return (np.arange(rows)[:, None] == origin[None, :]).astype(jnp.bfloat16)


def selectors(heads, nope, rope, slot):
    qk = nope + rope
    half = rope // 2

    def swapped(c):
        return c + half if nope <= c < nope + half else c - half if nope + half <= c < qk else -1

    def plain(h, c):
        return c + h * qk if c < qk else -1

    def turned(h, c):
        return swapped(c) + h * qk if nope <= c < qk else -1

    def shared(h, c):
        return -1 if c < nope or c >= qk else (swapped(c) if h else c) - nope

    query = np.concatenate(
        [
            selector(heads * qk, heads * slot, slot, plain),
            selector(heads * qk, heads * slot, slot, turned),
        ],
        axis=1,
    )
    key = selector(
        heads * nope, heads * slot, slot, lambda h, c: c + h * nope if c < nope else -1
    )
    return query, key, selector(rope, 2 * slot, slot, shared)


def trig(positions, nope, rope):
    frequency = 10000.0 ** (-2.0 * np.arange(rope // 2) / rope)
    angle = np.asarray(positions, np.float64)[:, None] * frequency[None, :]
    cos = np.ones((len(positions), 128))
    sin = np.zeros((len(positions), 128))
    cos[:, nope : nope + rope] = np.concatenate([np.cos(angle)] * 2, axis=1)
    sin[:, nope : nope + rope] = np.concatenate([np.sin(angle)] * 2, axis=1)
    return np.stack([cos, sin]).astype(np.float32)


def per_device(
    residual,
    query,
    latent,
    rope_key,
    latent_gain,
    query_gain,
    key_gain,
    key_weight,
    value_weight,
    mix_gain,
    out_weight,
    ffn_gain,
    expert_choice,
    group_prob,
    expert_prob,
    gate_weight,
    up_weight,
    down_weight,
):
    n_sp = lax.axis_size("sp")
    n_dp = lax.axis_size("dp")
    n_z = GROUPS
    n_y = n_sp // n_z
    tok, width = residual.shape[1:]
    rope = rope_key.shape[2]
    qk = query_gain.shape[0]
    nope = qk - rope
    lat = latent.shape[2]
    head_count = query.shape[2] // qk
    value_width = value_weight.shape[1] // head_count
    heads = head_count // n_z
    length = n_sp * tok
    half = rope // 2
    top = expert_choice.shape[2]
    peers = n_y * n_dp
    cap = tok // peers
    rows = tok // top
    hidden = gate_weight.shape[2]
    slot = 128
    wide_v = heads * value_width
    bf = jnp.bfloat16
    f32 = jnp.float32
    near = jnp.asarray(trig(np.arange(tok), nope, rope))
    far = jnp.asarray(trig(np.arange(n_sp) * tok, nope, rope))
    picks, spreads, ropes = [jnp.asarray(m) for m in selectors(heads, nope, rope, slot)]
    vmem = pltpu.VMEM
    hbm = pl.BlockSpec(memory_space=pl.ANY)
    dma = pltpu.SemaphoreType.DMA
    out = pl.pallas_call(
        functools.partial(
            layer_kernel, n_sp, n_y, n_dp, nope, rope, value_width, cap, top
        ),
        out_shape=jax.ShapeDtypeStruct((tok, width), bf),
        in_specs=[hbm] * 23,
        out_specs=pl.BlockSpec(memory_space=vmem),
        scratch_shapes=[
            vmem((tok, width), bf),
            vmem((tok, lat), bf),
            vmem((rope, tok), bf),
            vmem((1, lat), f32),
            vmem((1, qk), f32),
            vmem((1, qk), f32),
            vmem((lat, wide_v), bf),
            vmem((lat, wide_v), bf),
            vmem((1, head_count * value_width), f32),
            vmem(out_weight.shape, bf),
            vmem((1, width), f32),
            vmem((top, tok), jnp.int32),
            vmem((1, tok), f32),
            vmem((top, tok), f32),
            vmem((width, hidden), bf),
            vmem((width, hidden), bf),
            vmem((hidden, width), bf),
            vmem(near.shape, f32),
            vmem(far.shape, f32),
            vmem((lat, heads * slot), bf),
            vmem(picks.shape, bf),
            vmem(spreads.shape, bf),
            vmem(ropes.shape, bf),
            vmem((n_z, tok, heads * qk), bf),
            vmem((tok + half, lat), bf),
            vmem((n_sp, tok + half, lat), bf),
            vmem((n_z, heads, tok, slot), bf),
            vmem((heads, length, slot), bf),
            vmem((length, wide_v), bf),
            vmem((tok, n_y * tok), f32),
            vmem((heads * tok, length), bf),
            vmem((n_z, tok, wide_v), bf),
            vmem((n_z, tok, wide_v), bf),
            vmem((tok, width), bf),
            vmem((slot, tok), bf),
            vmem((n_z, rows, tok), bf),
            vmem((n_z, rows, width + slot), bf),
            vmem((n_z, rows, width + slot), bf),
            vmem((n_z, peers, cap, width), bf),
            vmem((n_z, peers, cap, width), bf),
            vmem((n_z, peers, cap, width), bf),
            vmem((n_z, peers, cap, width), bf),
            vmem((n_z, rows, width), bf),
            vmem((n_z, rows, width), bf),
            vmem((tok, width), f32),
            dma((23,)),
            dma((n_z,)),
            dma((n_z,)),
            dma((n_z,)),
            dma((n_z,)),
            dma((n_y,)),
            dma((n_y,)),
            dma((n_z, n_y)),
            dma((n_z, n_y)),
            dma((n_y, n_z)),
            dma((n_y, n_z)),
            dma((n_z,)),
            dma((n_z,)),
            dma((n_z,)),
            dma((n_z,)),
            dma((n_z, peers)),
            dma((n_z, peers)),
            dma((n_z, peers)),
            dma((n_z, peers)),
            dma((n_z,)),
            dma((n_z,)),
        ],
        compiler_params=pltpu.CompilerParams(
            collective_id=0, has_side_effects=True, vmem_limit_bytes=50 * 1024 * 1024
        ),
    )(
        *[pltpu.with_memory_space_constraint(v, pltpu.HBM) for v in (residual[0],
        query[0],
        latent[0],
        rope_key[0].T,
        latent_gain[None],
        query_gain[None],
        key_gain[None],
        key_weight,
        value_weight,
        mix_gain[None],
        out_weight,
        ffn_gain[None],
        expert_choice[0].T,
        group_prob,
        expert_prob[0].T,
        gate_weight[0],
        up_weight[0],
        down_weight[0],
        near,
        far,
        picks,
        spreads,
        ropes)],
    )
    return out[None]


def solution(mesh):
    return jax.shard_map(
        per_device,
        mesh=mesh,
        in_specs=(
            P("dp", "sp", None),
            P("dp", "sp", None),
            P("dp", "sp", None),
            P("dp", "sp", None),
            P(),
            P(),
            P(),
            P(),
            P(),
            P(),
            P(),
            P(),
            P("dp", "sp", None),
            P("dp", "sp"),
            P("dp", "sp", None),
            P(("sp", "dp"), None, None),
            P(("sp", "dp"), None, None),
            P(("sp", "dp"), None, None),
        ),
        out_specs=P("dp", "sp", None),
        check_vma=False,
    )
```

```python
import functools

import jax
import jax.numpy as jnp
import numpy as np
from jax import lax
from jax.experimental import pallas as pl
from jax.experimental.pallas import tpu as pltpu
from jax.sharding import PartitionSpec as P

GROUPS = 4
SPAN = 64


eps = 1e-06


def dot32(a, b):
    return jnp.dot(a, b, preferred_element_type=jnp.float32)


def dot_t(a, b):
    return lax.dot_general(a, b, (((0,), (0,)), ((), ())), preferred_element_type=jnp.float32)


def layer_kernel(
    n_sp,
    n_y,
    n_dp,
    nope,
    rope,
    value_width,
    cap,
    top,
    residual_hbm,
    query_hbm,
    latent_hbm,
    rope_t_hbm,
    latent_gain_hbm,
    query_gain_hbm,
    key_gain_hbm,
    key_weight_hbm,
    value_weight_hbm,
    mix_gain_hbm,
    out_weight_hbm,
    ffn_gain_hbm,
    choice_hbm,
    group_prob_hbm,
    share_hbm,
    gate_hbm,
    up_hbm,
    down_hbm,
    near_hbm,
    far_hbm,
    pick_query_hbm,
    spread_key_hbm,
    pick_rope_hbm,
    out_ref,
    residual_ref,
    latent_ref,
    rope_t_ref,
    latent_gain_ref,
    query_gain_ref,
    key_gain_ref,
    key_weight_ref,
    value_weight_ref,
    mix_gain_ref,
    out_weight_ref,
    ffn_gain_ref,
    choice_ref,
    group_prob_ref,
    share_ref,
    gate_ref,
    up_ref,
    down_ref,
    near_ref,
    far_ref,
    wide_key,
    pick_query,
    spread_key,
    pick_rope,
    queries_in,
    packed,
    packed_in,
    queries,
    keys,
    values,
    bias,
    weights,
    heads_out,
    token_in,
    normed_ref,
    info_ref,
    pick_ref,
    out1,
    in1,
    out2,
    arrive,
    served,
    back2,
    merged,
    home,
    acc,
    w_sem,
    sq,
    rq,
    sz,
    rz,
    sv,
    rv,
    sy,
    ry,
    sx,
    rx,
    so,
    ro,
    s1,
    r1,
    s2,
    r2,
    s3,
    r3,
    s4,
    r4,
):
    bf = jnp.bfloat16
    f32 = jnp.float32
    tok = latent_ref.shape[0]
    width = out_ref.shape[1]
    qk = nope + rope
    half = rope // 2
    n_z = n_sp // n_y
    heads = n_z
    slot = 128
    wide_q = heads * qk
    wide_v = heads * value_width
    me = lax.axis_index("sp")
    z = me // n_y
    y = me % n_y

    def query_part(target):
        return query_hbm.at[:, pl.ds(pl.multiple_of(target * wide_q, slot), wide_q)]

    own_part = pl.ds(pl.multiple_of(z * wide_v, slot), wide_v)
    pairs = [
        (latent_hbm, latent_ref),
        (latent_gain_hbm, latent_gain_ref),
        (rope_t_hbm, rope_t_ref),
        (key_weight_hbm.at[:, own_part], key_weight_ref),
        (value_weight_hbm.at[:, own_part], value_weight_ref),
        (near_hbm, near_ref),
        (pick_rope_hbm, pick_rope),
        (spread_key_hbm, spread_key),
        (pick_query_hbm, pick_query),
        (far_hbm, far_ref),
        (query_gain_hbm, query_gain_ref),
        (key_gain_hbm, key_gain_ref),
        (query_part(z), queries_in.at[z]),
        (choice_hbm, choice_ref),
        (group_prob_hbm, group_prob_ref),
        (share_hbm, share_ref),
        (mix_gain_hbm, mix_gain_ref),
        (ffn_gain_hbm, ffn_gain_ref),
        (residual_hbm, residual_ref),
        (out_weight_hbm, out_weight_ref),
        (gate_hbm, gate_ref),
        (up_hbm, up_ref),
        (down_hbm, down_ref),
    ]
    loads = [
        pltpu.make_async_copy(src, dst, w_sem.at[n]) for n, (src, dst) in enumerate(pairs)
    ]
    small = 18
    for load in loads[:small]:
        load.start()

    def remote(src, dst, send, recv, target):
        return pltpu.make_async_remote_copy(
            src_ref=src,
            dst_ref=dst,
            send_sem=send,
            recv_sem=recv,
            device_id=target if isinstance(target, dict) else {"sp": target},
            device_id_type=pl.DeviceIdType.MESH,
        )

    dp = lax.axis_index("dp")
    peers = n_y * n_dp
    rows = tok // top
    mine = y * n_dp + dp

    def peer(j):
        other = (mine + j) % peers
        return {"sp": z * n_y + other // n_dp, "dp": other % n_dp}

    def at_z(k):
        return ((z + k) % n_z) * n_y + y

    def at_y(m):
        return z * n_y + (y + m) % n_y

    barrier = pltpu.get_barrier_semaphore()
    greeted = [{"sp": at_z(k)} for k in range(1, n_z)] + [{"sp": at_y(m)} for m in range(1, n_y)]
    greeted += [{"dp": (dp + d) % n_dp} for d in range(1, n_dp)]
    for target in greeted:
        pl.semaphore_signal(
            barrier, inc=1, device_id=target, device_id_type=pl.DeviceIdType.MESH
        )
    for load in loads[:3]:
        load.wait()
    raw = latent_ref[...].astype(f32)
    scale = lax.rsqrt(jnp.mean(raw * raw, axis=-1, keepdims=True) + eps)
    packed[:tok] = (raw * scale * latent_gain_ref[...]).astype(bf)
    packed[tok:, :tok] = rope_t_ref[:half]
    packed[tok:, tok:] = rope_t_ref[half:]
    pl.semaphore_wait(barrier, len(greeted))

    sent = []
    asked = []
    down = {}
    over = {}
    cut = packed.shape[0] * 5 // 9

    def spread_y(k, source):
        origin = at_z(n_z - k) if k else me
        for m in (1, 3, 2):
            copy = remote(
                source, packed_in.at[origin, :cut], sy.at[k, m], ry.at[k, m], at_y(m)
            )
            copy.start()
            sent.append(copy)

    def spread_z(m, source):
        origin = at_y(n_y - m) if m else me
        for k in (1, 3, 2):
            copy = remote(
                source, packed_in.at[origin, cut:], sx.at[m, k], rx.at[m, k], at_z(k)
            )
            copy.start()
            sent.append(copy)

    def ask():
        for k in (1, 3, 2):
            target = (z + k) % n_z
            copy = remote(query_part(target), queries_in.at[z], sq.at[k], rq.at[k], at_z(k))
            copy.start()
            asked.append(copy)

    for k in (1, 3, 2):
        down[k] = remote(
            packed.at[:cut], packed_in.at[me, :cut], sz.at[k], rz.at[k], at_z(k)
        )
        down[k].start()
        over[k] = remote(
            packed.at[cut:], packed_in.at[me, cut:], sv.at[k], rv.at[k], at_y(k)
        )
        over[k].start()
    spread_y(0, packed.at[:cut])
    spread_z(0, packed.at[cut:])
    packed_in[me] = packed[...]

    def route():
        lower = lax.broadcasted_iota(jnp.int32, (tok, tok), 0)
        upper = lax.broadcasted_iota(jnp.int32, (tok, tok), 1)
        before = (lower < upper).astype(f32).astype(bf)
        per_group = peers
        chosen = choice_ref[...]
        group = chosen[0:1] // per_group
        of_group = (
            lax.broadcasted_iota(jnp.int32, (8, tok), 0) == jnp.broadcast_to(group, (8, tok))
        ).astype(f32)
        rank = jnp.sum(of_group * dot32(of_group.astype(bf), before), axis=0, keepdims=True)
        line = group * rows + rank.astype(jnp.int32)
        place = lax.broadcasted_iota(jnp.int32, (n_z * rows, tok), 0)
        pick = (place == jnp.broadcast_to(line, place.shape)).astype(f32).astype(bf)
        for g in range(n_z):
            pick_ref[g] = pick[g * rows : (g + 1) * rows]
        expert = lax.broadcasted_iota(jnp.int32, (n_z * per_group, tok), 0)
        of_expert = [
            (expert == jnp.broadcast_to(chosen[t : t + 1], expert.shape)).astype(f32)
            for t in range(top)
        ]
        named = of_expert[0]
        for t in range(1, top):
            named = named + of_expert[t]
        count = dot32(named.astype(bf), before)
        share = share_ref[...]
        whole = share[0:1]
        for t in range(1, top):
            whole = whole + share[t : t + 1]
        lines = []
        for t in range(top):
            earlier = jnp.sum(of_expert[t] * count, axis=0, keepdims=True)
            local_one = ((chosen[t : t + 1] - group * per_group) * cap).astype(f32)
            lines.append(local_one + earlier)
        for t in range(top):
            part = group_prob_ref[...] * share[t : t + 1] / whole
            high = part.astype(bf).astype(f32)
            lines += [high, part - high]
        at = lax.broadcasted_iota(jnp.int32, (slot, tok), 0)
        total = jnp.zeros((slot, tok), f32)
        for n, values_of in enumerate(lines):
            total = jnp.where(at == n, jnp.broadcast_to(values_of, at.shape), total)
        info_ref[...] = total.astype(bf)

    gaps = [(1, 1), (3, 3), (2, 2)]
    for k, m in gaps:
        down[k].wait_recv()
        spread_y(k, packed_in.at[at_z(n_z - k), :cut])
        over[m].wait_recv()
        spread_z(m, packed_in.at[at_y(n_y - m), cut:])
    ask()

    for load in loads[small:]:
        load.start()
    for load in loads[3:small]:
        load.wait()
    q_pos = y * tok + lax.broadcasted_iota(jnp.int32, bias.shape, 0)
    k_pos = lax.broadcasted_iota(jnp.int32, bias.shape, 1)
    bias[...] = jnp.where(k_pos // SPAN <= q_pos // SPAN, 0.0, -1e30)
    wide_key[...] = dot32(key_weight_ref[...], spread_key[...]).astype(bf)
    route()

    near_cos, near_sin = near_ref[0], near_ref[1]

    def tables(block):
        far_cos = far_ref[0, pl.ds(block, 1), :]
        far_sin = far_ref[1, pl.ds(block, 1), :]
        return (
            far_cos * near_cos - far_sin * near_sin,
            far_sin * near_cos + far_cos * near_sin,
        )

    def both(gain_ref):
        gain = jnp.concatenate([gain_ref[...], jnp.zeros((1, slot - qk), f32)], axis=1)
        gain = jnp.broadcast_to(gain, (8, slot))
        c = lax.broadcasted_iota(jnp.int32, (8, slot), 1)
        up = pltpu.roll(gain, half, 1)
        down_by = pltpu.roll(gain, slot - half, 1)
        turned = jnp.where(
            c < nope, 0.0, jnp.where(c < nope + half, -down_by, jnp.where(c < qk, up, 0.0))
        )
        return gain[0:1], turned[0:1]

    query_gain, query_swap = both(query_gain_ref)
    key_gain, key_swap = both(key_gain_ref)

    def prepare(i, carry):
        step = i // n_y
        k = jnp.where(step < 2, step, 5 - step)
        m = i % n_y
        origin = (z + n_z - k) % n_z
        s = origin * n_y + (y + n_y - m) % n_y

        @pl.when(m > 0)
        def _():
            part = packed_in.at[s, :cut]
            remote(part, part, sy.at[k, m], ry.at[k, m], me).wait_recv()

        @pl.when(k > 0)
        def _():
            part = packed_in.at[s, cut:]
            remote(part, part, sx.at[m, k], rx.at[m, k], me).wait_recv()

        at = pl.ds(pl.multiple_of(s * tok, tok), tok)
        block = packed_in[s]
        latent = block[:tok]
        values[at, :] = dot32(latent, value_weight_ref[...]).astype(bf)
        part = dot32(latent, wide_key[...]).astype(bf).astype(f32)
        turned_rows = jnp.concatenate([block[tok:, :tok], block[tok:, tok:]], axis=0)
        spun = dot_t(turned_rows, pick_rope[...])
        cos, sin = tables(s)
        plain_rope = spun[:, :slot]
        tail = plain_rope * (key_gain * cos) + spun[:, slot:] * (key_swap * sin)
        for h in range(heads):
            own = part[:, h * slot : (h + 1) * slot]
            full = own + plain_rope
            norm = lax.rsqrt(jnp.sum(full * full, axis=-1, keepdims=True) / qk + eps)
            keys[h, at, :] = ((own * key_gain + tail) * norm).astype(bf)
        return carry

    lax.fori_loop(0, n_sp, prepare, 0)

    for copy in asked:
        copy.wait_recv()

    def prepare_queries(b, carry):
        raw = queries_in[b]
        both_parts = dot32(raw, pick_query[...])
        plain, turned = both_parts[:, : heads * slot], both_parts[:, heads * slot :]
        cos, sin = tables(b * n_y + y)
        for h in range(heads):
            span = slice(h * slot, (h + 1) * slot)
            own = plain[:, span]
            norm = lax.rsqrt(jnp.sum(own * own, axis=-1, keepdims=True) / qk + eps)
            queries[b, h] = (
                (own * (query_gain * cos) + turned[:, span] * (query_swap * sin)) * norm
            ).astype(bf)
        return carry

    lax.fori_loop(0, n_z, prepare_queries, 0)

    stretch = n_y * tok
    factor = qk ** (-0.5) * 1.4426950408889634
    lane = lax.broadcasted_iota(jnp.int32, (tok, wide_v), 1) // value_width
    for b in range(n_z - 1, -1, -1):
        last = (b + 1) * stretch
        sums = []
        for h in range(heads):
            scores = lax.dot_general(
                queries[b, h],
                keys[h, :last],
                (((1,), (1,)), ((), ())),
                preferred_element_type=f32,
            )
            edge = scores[:, last - stretch :] + bias[...]
            top = jnp.max(edge, axis=-1, keepdims=True)
            if b:
                inner = scores[:, : last - stretch]
                top = jnp.maximum(top, jnp.max(inner, axis=-1, keepdims=True))
            raised = jnp.exp2((edge - top) * factor)
            total = jnp.sum(raised, axis=-1, keepdims=True)
            weights[h * tok : (h + 1) * tok, last - stretch : last] = raised.astype(bf)
            if b:
                raised = jnp.exp2((inner - top) * factor)
                total = total + jnp.sum(raised, axis=-1, keepdims=True)
                weights[h * tok : (h + 1) * tok, : last - stretch] = raised.astype(bf)
            sums.append(total)
        mixed = dot32(weights[:, :last], values[:last])
        total = None
        for h in range(heads):
            own = mixed[h * tok : (h + 1) * tok] / sums[h]
            total = own if total is None else jnp.where(lane < h, total, own)
        heads_out[b] = total.astype(bf)
        if b == 0:
            for done in range(n_z - 1, -1, -1):

                @pl.when(z != done)
                def _():
                    remote(
                        heads_out.at[done], token_in.at[z], so.at[done], ro.at[z], done * n_y + y
                    ).start()

    token_in[z] = heads_out[z]
    for load in loads[small:]:
        load.wait()
    for k in range(1, n_z):
        other = (z + k) % n_z
        remote(
            heads_out.at[other], token_in.at[other], so.at[other], ro.at[other], other * n_y + y
        ).wait()
    square = None
    for s in range(n_z):
        piece = token_in[s].astype(f32)
        part = jnp.sum(piece * piece, axis=-1, keepdims=True)
        square = part if square is None else square + part
    scale = lax.rsqrt(square / (n_z * wide_v) + eps)
    mixed = jnp.concatenate(
        [
            (token_in[s].astype(f32) * scale * mix_gain_ref[:, s * wide_v : (s + 1) * wide_v]).astype(bf)
            for s in range(n_z)
        ],
        axis=1,
    )
    stream = residual_ref[...].astype(f32) + dot32(mixed, out_weight_ref[...])
    acc[...] = stream
    scale = lax.rsqrt(jnp.mean(stream * stream, axis=-1, keepdims=True) + eps)
    normed_ref[...] = (stream * scale * ffn_gain_ref[...]).astype(bf)

    first = {}

    def pack(k, target):
        picks = pick_ref[(z + k) % n_z]
        target[k, :, :width] = dot32(picks, normed_ref[...]).astype(bf)
        target[k, :, width:] = lax.dot_general(
            picks, info_ref[...], (((1,), (1,)), ((), ())), preferred_element_type=f32
        ).astype(bf)

    def launch(k):
        pack(k, out1)
        first[k] = remote(out1.at[k], in1.at[k], s1.at[k], r1.at[k], at_z(k))
        first[k].start()

    def slots(k):
        info = in1[k, :, width:].astype(f32)
        place = lax.broadcasted_iota(jnp.int32, (rows, peers * cap), 1).astype(f32)
        return place == info[:, 0:1], place == info[:, 1:2], info

    second = {}

    def scatter(k):
        if k:
            first[k].wait_recv()
        at0, at1, _ = slots(k)
        choose = (at0.astype(f32) + at1.astype(f32)).astype(bf)
        placed = dot_t(choose, in1[k, :, :width]).astype(bf)
        for e in range(peers):
            out2[k, e] = placed[e * cap : (e + 1) * cap]
        second[k] = [
            remote(
                out2.at[k, (mine + j) % peers], arrive.at[k, j], s2.at[k, j], r2.at[k, j], peer(j)
            )
            for j in range(1, peers)
        ]
        for copy in second[k]:
            copy.start()
        arrive[k, 0] = out2[k, mine]

    third = {}

    def serve(k):
        for copy in second[k]:
            copy.wait_recv()
        given = arrive[k].reshape(peers * cap, width)
        gate_act = dot32(given, gate_ref[...])
        upward = dot32(given, up_ref[...])
        hidden = (gate_act * (1.0 / (1.0 + jnp.exp(-gate_act))) * upward).astype(bf)
        result = dot32(hidden, down_ref[...]).astype(bf)
        for j in range(peers):
            served[k, j] = result[j * cap : (j + 1) * cap]
        third[k] = [
            remote(
                served.at[k, j], back2.at[k, mine], s3.at[k, j], r3.at[k, peers - j], peer(peers - j)
            )
            for j in range(1, peers)
        ]
        for copy in third[k]:
            copy.start()
        back2[k, mine] = served[k, 0]

    fourth = {}

    def merge(k):
        for copy in third[k]:
            copy.wait_recv()
        at0, at1, info = slots(k)
        high = jnp.where(at0, info[:, 2:3], 0.0) + jnp.where(at1, info[:, 4:5], 0.0)
        low = jnp.where(at0, info[:, 3:4], 0.0) + jnp.where(at1, info[:, 5:6], 0.0)
        got = back2[k].reshape(peers * cap, width)
        total = dot32(high.astype(bf), got) + dot32(low.astype(bf), got)
        if k:
            merged[k] = total.astype(bf)
            fourth[k] = remote(merged.at[k], home.at[k], s4.at[k], r4.at[k], at_z(n_z - k))
            fourth[k].start()
        else:
            acc[...] += dot_t(pick_ref[z], total.astype(bf))

    pack(0, in1)
    launch(1)
    scatter(0)
    launch(3)
    launch(2)
    for k in (1, 3, 2):
        scatter(k)
    for k in (1, 3, 2, 0):
        serve(k)
    for k in (1, 3, 2, 0):
        merge(k)
    for k in (1, 3, 2):
        fourth[k].wait_recv()
        acc[...] += dot_t(pick_ref[(z + k) % n_z], home[k])
    out_ref[...] = acc[...].astype(bf)
    for copy in list(down.values()) + list(over.values()) + sent + asked:
        copy.wait_send()
    for k in range(n_z):
        if k:
            first[k].wait_send()
            fourth[k].wait_send()
        for copy in second[k] + third[k]:
            copy.wait_send()


def selector(rows, columns, slot, source):
    head, lane = np.divmod(np.arange(columns), slot)
    origin = np.asarray([source(h, c) for h, c in zip(head, lane)])
    return (np.arange(rows)[:, None] == origin[None, :]).astype(jnp.bfloat16)


def selectors(heads, nope, rope, slot):
    qk = nope + rope
    half = rope // 2

    def swapped(c):
        return c + half if nope <= c < nope + half else c - half if nope + half <= c < qk else -1

    def plain(h, c):
        return c + h * qk if c < qk else -1

    def turned(h, c):
        return swapped(c) + h * qk if nope <= c < qk else -1

    def shared(h, c):
        return -1 if c < nope or c >= qk else (swapped(c) if h else c) - nope

    query = np.concatenate(
        [
            selector(heads * qk, heads * slot, slot, plain),
            selector(heads * qk, heads * slot, slot, turned),
        ],
        axis=1,
    )
    key = selector(
        heads * nope, heads * slot, slot, lambda h, c: c + h * nope if c < nope else -1
    )
    return query, key, selector(rope, 2 * slot, slot, shared)


def trig(positions, nope, rope):
    frequency = 10000.0 ** (-2.0 * np.arange(rope // 2) / rope)
    angle = np.asarray(positions, np.float64)[:, None] * frequency[None, :]
    cos = np.ones((len(positions), 128))
    sin = np.zeros((len(positions), 128))
    cos[:, nope : nope + rope] = np.concatenate([np.cos(angle)] * 2, axis=1)
    sin[:, nope : nope + rope] = np.concatenate([np.sin(angle)] * 2, axis=1)
    return np.stack([cos, sin]).astype(np.float32)


def per_device(
    residual,
    query,
    latent,
    rope_key,
    latent_gain,
    query_gain,
    key_gain,
    key_weight,
    value_weight,
    mix_gain,
    out_weight,
    ffn_gain,
    expert_choice,
    group_prob,
    expert_prob,
    gate_weight,
    up_weight,
    down_weight,
):
    n_sp = lax.axis_size("sp")
    n_dp = lax.axis_size("dp")
    n_z = GROUPS
    n_y = n_sp // n_z
    tok, width = residual.shape[1:]
    rope = rope_key.shape[2]
    qk = query_gain.shape[0]
    nope = qk - rope
    lat = latent.shape[2]
    head_count = query.shape[2] // qk
    value_width = value_weight.shape[1] // head_count
    heads = head_count // n_z
    length = n_sp * tok
    half = rope // 2
    top = expert_choice.shape[2]
    peers = n_y * n_dp
    cap = tok // peers
    rows = tok // top
    hidden = gate_weight.shape[2]
    slot = 128
    wide_v = heads * value_width
    bf = jnp.bfloat16
    f32 = jnp.float32
    near = jnp.asarray(trig(np.arange(tok), nope, rope))
    far = jnp.asarray(trig(np.arange(n_sp) * tok, nope, rope))
    picks, spreads, ropes = [jnp.asarray(m) for m in selectors(heads, nope, rope, slot)]
    vmem = pltpu.VMEM
    hbm = pl.BlockSpec(memory_space=pl.ANY)
    dma = pltpu.SemaphoreType.DMA
    out = pl.pallas_call(
        functools.partial(
            layer_kernel, n_sp, n_y, n_dp, nope, rope, value_width, cap, top
        ),
        out_shape=jax.ShapeDtypeStruct((tok, width), bf),
        in_specs=[hbm] * 23,
        out_specs=pl.BlockSpec(memory_space=vmem),
        scratch_shapes=[
            vmem((tok, width), bf),
            vmem((tok, lat), bf),
            vmem((rope, tok), bf),
            vmem((1, lat), f32),
            vmem((1, qk), f32),
            vmem((1, qk), f32),
            vmem((lat, wide_v), bf),
            vmem((lat, wide_v), bf),
            vmem((1, head_count * value_width), f32),
            vmem(out_weight.shape, bf),
            vmem((1, width), f32),
            vmem((top, tok), jnp.int32),
            vmem((1, tok), f32),
            vmem((top, tok), f32),
            vmem((width, hidden), bf),
            vmem((width, hidden), bf),
            vmem((hidden, width), bf),
            vmem(near.shape, f32),
            vmem(far.shape, f32),
            vmem((lat, heads * slot), bf),
            vmem(picks.shape, bf),
            vmem(spreads.shape, bf),
            vmem(ropes.shape, bf),
            vmem((n_z, tok, heads * qk), bf),
            vmem((tok + half, lat), bf),
            vmem((n_sp, tok + half, lat), bf),
            vmem((n_z, heads, tok, slot), bf),
            vmem((heads, length, slot), bf),
            vmem((length, wide_v), bf),
            vmem((tok, n_y * tok), f32),
            vmem((heads * tok, length), bf),
            vmem((n_z, tok, wide_v), bf),
            vmem((n_z, tok, wide_v), bf),
            vmem((tok, width), bf),
            vmem((slot, tok), bf),
            vmem((n_z, rows, tok), bf),
            vmem((n_z, rows, width + slot), bf),
            vmem((n_z, rows, width + slot), bf),
            vmem((n_z, peers, cap, width), bf),
            vmem((n_z, peers, cap, width), bf),
            vmem((n_z, peers, cap, width), bf),
            vmem((n_z, peers, cap, width), bf),
            vmem((n_z, rows, width), bf),
            vmem((n_z, rows, width), bf),
            vmem((tok, width), f32),
            dma((23,)),
            dma((n_z,)),
            dma((n_z,)),
            dma((n_z,)),
            dma((n_z,)),
            dma((n_y,)),
            dma((n_y,)),
            dma((n_z, n_y)),
            dma((n_z, n_y)),
            dma((n_y, n_z)),
            dma((n_y, n_z)),
            dma((n_z,)),
            dma((n_z,)),
            dma((n_z,)),
            dma((n_z,)),
            dma((n_z, peers)),
            dma((n_z, peers)),
            dma((n_z, peers)),
            dma((n_z, peers)),
            dma((n_z,)),
            dma((n_z,)),
        ],
        compiler_params=pltpu.CompilerParams(
            collective_id=0, has_side_effects=True, vmem_limit_bytes=50 * 1024 * 1024
        ),
    )(
        *[pltpu.with_memory_space_constraint(v, pltpu.HBM) for v in (residual[0],
        query[0],
        latent[0],
        rope_key[0].T,
        latent_gain[None],
        query_gain[None],
        key_gain[None],
        key_weight,
        value_weight,
        mix_gain[None],
        out_weight,
        ffn_gain[None],
        expert_choice[0].T,
        group_prob,
        expert_prob[0].T,
        gate_weight[0],
        up_weight[0],
        down_weight[0],
        near,
        far,
        picks,
        spreads,
        ropes)],
    )
    return out[None]


def solution(mesh):
    return jax.shard_map(
        per_device,
        mesh=mesh,
        in_specs=(
            P("dp", "sp", None),
            P("dp", "sp", None),
            P("dp", "sp", None),
            P("dp", "sp", None),
            P(),
            P(),
            P(),
            P(),
            P(),
            P(),
            P(),
            P(),
            P("dp", "sp", None),
            P("dp", "sp"),
            P("dp", "sp", None),
            P(("sp", "dp"), None, None),
            P(("sp", "dp"), None, None),
            P(("sp", "dp"), None, None),
        ),
        out_specs=P("dp", "sp", None),
        check_vma=False,
    )
```

```python
import functools

import jax
import jax.numpy as jnp
import numpy as np
from jax import lax
from jax.experimental import pallas as pl
from jax.experimental.pallas import tpu as pltpu
from jax.sharding import PartitionSpec as P

GROUPS = 4
SPAN = 64


eps = 1e-06


def dot32(a, b):
    return jnp.dot(a, b, preferred_element_type=jnp.float32)


def dot_t(a, b):
    return lax.dot_general(a, b, (((0,), (0,)), ((), ())), preferred_element_type=jnp.float32)


def layer_kernel(
    n_sp,
    n_y,
    n_dp,
    nope,
    rope,
    value_width,
    cap,
    top,
    residual_hbm,
    query_hbm,
    latent_hbm,
    rope_t_hbm,
    latent_gain_hbm,
    query_gain_hbm,
    key_gain_hbm,
    key_weight_hbm,
    value_weight_hbm,
    mix_gain_hbm,
    out_weight_hbm,
    ffn_gain_hbm,
    choice_hbm,
    group_prob_hbm,
    share_hbm,
    gate_hbm,
    up_hbm,
    down_hbm,
    near_hbm,
    far_hbm,
    pick_query_hbm,
    spread_key_hbm,
    pick_rope_hbm,
    out_ref,
    residual_ref,
    latent_ref,
    rope_t_ref,
    latent_gain_ref,
    query_gain_ref,
    key_gain_ref,
    key_weight_ref,
    value_weight_ref,
    mix_gain_ref,
    out_weight_ref,
    ffn_gain_ref,
    choice_ref,
    group_prob_ref,
    share_ref,
    gate_ref,
    up_ref,
    down_ref,
    near_ref,
    far_ref,
    wide_key,
    pick_query,
    spread_key,
    pick_rope,
    queries_in,
    packed,
    packed_in,
    queries,
    keys,
    values,
    bias,
    weights,
    heads_out,
    token_in,
    normed_ref,
    info_ref,
    pick_ref,
    out1,
    in1,
    out2,
    arrive,
    served,
    back2,
    merged,
    home,
    acc,
    w_sem,
    sq,
    rq,
    sz,
    rz,
    sv,
    rv,
    sy,
    ry,
    sx,
    rx,
    so,
    ro,
    s1,
    r1,
    s2,
    r2,
    s3,
    r3,
    s4,
    r4,
):
    bf = jnp.bfloat16
    f32 = jnp.float32
    tok = latent_ref.shape[0]
    width = out_ref.shape[1]
    qk = nope + rope
    half = rope // 2
    n_z = n_sp // n_y
    heads = n_z
    slot = 128
    wide_q = heads * qk
    wide_v = heads * value_width
    me = lax.axis_index("sp")
    z = me // n_y
    y = me % n_y

    def query_part(target):
        return query_hbm.at[:, pl.ds(pl.multiple_of(target * wide_q, slot), wide_q)]

    own_part = pl.ds(pl.multiple_of(z * wide_v, slot), wide_v)
    pairs = [
        (latent_hbm, latent_ref),
        (latent_gain_hbm, latent_gain_ref),
        (rope_t_hbm, rope_t_ref),
        (key_weight_hbm.at[:, own_part], key_weight_ref),
        (value_weight_hbm.at[:, own_part], value_weight_ref),
        (near_hbm, near_ref),
        (pick_rope_hbm, pick_rope),
        (spread_key_hbm, spread_key),
        (pick_query_hbm, pick_query),
        (far_hbm, far_ref),
        (query_gain_hbm, query_gain_ref),
        (key_gain_hbm, key_gain_ref),
        (query_part(z), queries_in.at[z]),
        (choice_hbm, choice_ref),
        (group_prob_hbm, group_prob_ref),
        (share_hbm, share_ref),
        (mix_gain_hbm, mix_gain_ref),
        (ffn_gain_hbm, ffn_gain_ref),
        (residual_hbm, residual_ref),
        (out_weight_hbm, out_weight_ref),
        (gate_hbm, gate_ref),
        (up_hbm, up_ref),
        (down_hbm, down_ref),
    ]
    loads = [
        pltpu.make_async_copy(src, dst, w_sem.at[n]) for n, (src, dst) in enumerate(pairs)
    ]
    small = 18
    for load in loads[:small]:
        load.start()

    def remote(src, dst, send, recv, target):
        return pltpu.make_async_remote_copy(
            src_ref=src,
            dst_ref=dst,
            send_sem=send,
            recv_sem=recv,
            device_id=target if isinstance(target, dict) else {"sp": target},
            device_id_type=pl.DeviceIdType.MESH,
        )

    dp = lax.axis_index("dp")
    peers = n_y * n_dp
    rows = tok // top
    mine = y * n_dp + dp

    def peer(j):
        other = (mine + j) % peers
        return {"sp": z * n_y + other // n_dp, "dp": other % n_dp}

    def at_z(k):
        return ((z + k) % n_z) * n_y + y

    def at_y(m):
        return z * n_y + (y + m) % n_y

    barrier = pltpu.get_barrier_semaphore()
    greeted = [{"sp": at_z(k)} for k in range(1, n_z)] + [{"sp": at_y(m)} for m in range(1, n_y)]
    greeted += [{"dp": (dp + d) % n_dp} for d in range(1, n_dp)]
    for target in greeted:
        pl.semaphore_signal(
            barrier, inc=1, device_id=target, device_id_type=pl.DeviceIdType.MESH
        )
    for load in loads[:3]:
        load.wait()
    raw = latent_ref[...].astype(f32)
    scale = lax.rsqrt(jnp.mean(raw * raw, axis=-1, keepdims=True) + eps)
    packed[:tok] = (raw * scale * latent_gain_ref[...]).astype(bf)
    packed[tok:, :tok] = rope_t_ref[:half]
    packed[tok:, tok:] = rope_t_ref[half:]
    pl.semaphore_wait(barrier, len(greeted))

    sent = []
    asked = []
    down = {}
    over = {}
    cut = packed.shape[0] * 5 // 9

    def spread_y(k, source):
        origin = at_z(n_z - k) if k else me
        for m in (1, 3, 2):
            copy = remote(
                source, packed_in.at[origin, :cut], sy.at[k, m], ry.at[k, m], at_y(m)
            )
            copy.start()
            sent.append(copy)

    def spread_z(m, source):
        origin = at_y(n_y - m) if m else me
        for k in (1, 3, 2):
            copy = remote(
                source, packed_in.at[origin, cut:], sx.at[m, k], rx.at[m, k], at_z(k)
            )
            copy.start()
            sent.append(copy)

    def ask():
        for k in (1, 3, 2):
            target = (z + k) % n_z
            copy = remote(query_part(target), queries_in.at[z], sq.at[k], rq.at[k], at_z(k))
            copy.start()
            asked.append(copy)

    for k in (1, 3, 2):
        down[k] = remote(
            packed.at[:cut], packed_in.at[me, :cut], sz.at[k], rz.at[k], at_z(k)
        )
        down[k].start()
        over[k] = remote(
            packed.at[cut:], packed_in.at[me, cut:], sv.at[k], rv.at[k], at_y(k)
        )
        over[k].start()
    spread_z(0, packed.at[cut:])
    spread_y(0, packed.at[:cut])
    packed_in[me] = packed[...]

    def route():
        lower = lax.broadcasted_iota(jnp.int32, (tok, tok), 0)
        upper = lax.broadcasted_iota(jnp.int32, (tok, tok), 1)
        before = (lower < upper).astype(f32).astype(bf)
        per_group = peers
        chosen = choice_ref[...]
        group = chosen[0:1] // per_group
        of_group = (
            lax.broadcasted_iota(jnp.int32, (8, tok), 0) == jnp.broadcast_to(group, (8, tok))
        ).astype(f32)
        rank = jnp.sum(of_group * dot32(of_group.astype(bf), before), axis=0, keepdims=True)
        line = group * rows + rank.astype(jnp.int32)
        place = lax.broadcasted_iota(jnp.int32, (n_z * rows, tok), 0)
        pick = (place == jnp.broadcast_to(line, place.shape)).astype(f32).astype(bf)
        for g in range(n_z):
            pick_ref[g] = pick[g * rows : (g + 1) * rows]
        expert = lax.broadcasted_iota(jnp.int32, (n_z * per_group, tok), 0)
        of_expert = [
            (expert == jnp.broadcast_to(chosen[t : t + 1], expert.shape)).astype(f32)
            for t in range(top)
        ]
        named = of_expert[0]
        for t in range(1, top):
            named = named + of_expert[t]
        count = dot32(named.astype(bf), before)
        share = share_ref[...]
        whole = share[0:1]
        for t in range(1, top):
            whole = whole + share[t : t + 1]
        lines = []
        for t in range(top):
            earlier = jnp.sum(of_expert[t] * count, axis=0, keepdims=True)
            local_one = ((chosen[t : t + 1] - group * per_group) * cap).astype(f32)
            lines.append(local_one + earlier)
        for t in range(top):
            part = group_prob_ref[...] * share[t : t + 1] / whole
            high = part.astype(bf).astype(f32)
            lines += [high, part - high]
        at = lax.broadcasted_iota(jnp.int32, (slot, tok), 0)
        total = jnp.zeros((slot, tok), f32)
        for n, values_of in enumerate(lines):
            total = jnp.where(at == n, jnp.broadcast_to(values_of, at.shape), total)
        info_ref[...] = total.astype(bf)

    gaps = [(1, 1), (3, 3), (2, 2)]
    for k, m in gaps:
        down[k].wait_recv()
        spread_y(k, packed_in.at[at_z(n_z - k), :cut])
        over[m].wait_recv()
        spread_z(m, packed_in.at[at_y(n_y - m), cut:])
    ask()

    for load in loads[3:small]:
        load.wait()
    q_pos = y * tok + lax.broadcasted_iota(jnp.int32, bias.shape, 0)
    k_pos = lax.broadcasted_iota(jnp.int32, bias.shape, 1)
    bias[...] = jnp.where(k_pos // SPAN <= q_pos // SPAN, 0.0, -1e30)
    wide_key[...] = dot32(key_weight_ref[...], spread_key[...]).astype(bf)
    route()

    near_cos, near_sin = near_ref[0], near_ref[1]

    def tables(block):
        far_cos = far_ref[0, pl.ds(block, 1), :]
        far_sin = far_ref[1, pl.ds(block, 1), :]
        return (
            far_cos * near_cos - far_sin * near_sin,
            far_sin * near_cos + far_cos * near_sin,
        )

    def both(gain_ref):
        gain = jnp.concatenate([gain_ref[...], jnp.zeros((1, slot - qk), f32)], axis=1)
        gain = jnp.broadcast_to(gain, (8, slot))
        c = lax.broadcasted_iota(jnp.int32, (8, slot), 1)
        up = pltpu.roll(gain, half, 1)
        down_by = pltpu.roll(gain, slot - half, 1)
        turned = jnp.where(
            c < nope, 0.0, jnp.where(c < nope + half, -down_by, jnp.where(c < qk, up, 0.0))
        )
        return gain[0:1], turned[0:1]

    query_gain, query_swap = both(query_gain_ref)
    key_gain, key_swap = both(key_gain_ref)

    def prepare(i, carry):
        step = i // n_y
        k = jnp.where(step < 2, step, 5 - step)
        m = i % n_y
        origin = (z + n_z - k) % n_z
        s = origin * n_y + (y + n_y - m) % n_y

        @pl.when(m > 0)
        def _():
            part = packed_in.at[s, :cut]
            remote(part, part, sy.at[k, m], ry.at[k, m], me).wait_recv()

        @pl.when(k > 0)
        def _():
            part = packed_in.at[s, cut:]
            remote(part, part, sx.at[m, k], rx.at[m, k], me).wait_recv()

        at = pl.ds(pl.multiple_of(s * tok, tok), tok)
        block = packed_in[s]
        latent = block[:tok]
        values[at, :] = dot32(latent, value_weight_ref[...]).astype(bf)
        part = dot32(latent, wide_key[...]).astype(bf).astype(f32)
        turned_rows = jnp.concatenate([block[tok:, :tok], block[tok:, tok:]], axis=0)
        spun = dot_t(turned_rows, pick_rope[...])
        cos, sin = tables(s)
        plain_rope = spun[:, :slot]
        tail = plain_rope * (key_gain * cos) + spun[:, slot:] * (key_swap * sin)
        for h in range(heads):
            own = part[:, h * slot : (h + 1) * slot]
            full = own + plain_rope
            norm = lax.rsqrt(jnp.sum(full * full, axis=-1, keepdims=True) / qk + eps)
            keys[h, at, :] = ((own * key_gain + tail) * norm).astype(bf)
        return carry

    lax.fori_loop(0, n_sp, prepare, 0)
    for load in loads[small:]:
        load.start()

    for copy in asked:
        copy.wait_recv()

    def prepare_queries(b, carry):
        raw = queries_in[b]
        both_parts = dot32(raw, pick_query[...])
        plain, turned = both_parts[:, : heads * slot], both_parts[:, heads * slot :]
        cos, sin = tables(b * n_y + y)
        for h in range(heads):
            span = slice(h * slot, (h + 1) * slot)
            own = plain[:, span]
            norm = lax.rsqrt(jnp.sum(own * own, axis=-1, keepdims=True) / qk + eps)
            queries[b, h] = (
                (own * (query_gain * cos) + turned[:, span] * (query_swap * sin)) * norm
            ).astype(bf)
        return carry

    lax.fori_loop(0, n_z, prepare_queries, 0)

    stretch = n_y * tok
    factor = qk ** (-0.5) * 1.4426950408889634
    lane = lax.broadcasted_iota(jnp.int32, (tok, wide_v), 1) // value_width
    for b in range(n_z - 1, -1, -1):
        last = (b + 1) * stretch
        sums = []
        for h in range(heads):
            scores = lax.dot_general(
                queries[b, h],
                keys[h, :last],
                (((1,), (1,)), ((), ())),
                preferred_element_type=f32,
            )
            edge = scores[:, last - stretch :] + bias[...]
            top = jnp.max(edge, axis=-1, keepdims=True)
            if b:
                inner = scores[:, : last - stretch]
                top = jnp.maximum(top, jnp.max(inner, axis=-1, keepdims=True))
            raised = jnp.exp2((edge - top) * factor)
            total = jnp.sum(raised, axis=-1, keepdims=True)
            weights[h * tok : (h + 1) * tok, last - stretch : last] = raised.astype(bf)
            if b:
                raised = jnp.exp2((inner - top) * factor)
                total = total + jnp.sum(raised, axis=-1, keepdims=True)
                weights[h * tok : (h + 1) * tok, : last - stretch] = raised.astype(bf)
            sums.append(total)
        mixed = dot32(weights[:, :last], values[:last])
        total = None
        for h in range(heads):
            own = mixed[h * tok : (h + 1) * tok] / sums[h]
            total = own if total is None else jnp.where(lane < h, total, own)
        heads_out[b] = total.astype(bf)
        if b == 0:
            for done in range(n_z - 1, -1, -1):

                @pl.when(z != done)
                def _():
                    remote(
                        heads_out.at[done], token_in.at[z], so.at[done], ro.at[z], done * n_y + y
                    ).start()

    token_in[z] = heads_out[z]
    for load in loads[small:]:
        load.wait()
    for k in range(1, n_z):
        other = (z + k) % n_z
        remote(
            heads_out.at[other], token_in.at[other], so.at[other], ro.at[other], other * n_y + y
        ).wait()
    square = None
    for s in range(n_z):
        piece = token_in[s].astype(f32)
        part = jnp.sum(piece * piece, axis=-1, keepdims=True)
        square = part if square is None else square + part
    scale = lax.rsqrt(square / (n_z * wide_v) + eps)
    mixed = jnp.concatenate(
        [
            (token_in[s].astype(f32) * scale * mix_gain_ref[:, s * wide_v : (s + 1) * wide_v]).astype(bf)
            for s in range(n_z)
        ],
        axis=1,
    )
    stream = residual_ref[...].astype(f32) + dot32(mixed, out_weight_ref[...])
    acc[...] = stream
    scale = lax.rsqrt(jnp.mean(stream * stream, axis=-1, keepdims=True) + eps)
    normed_ref[...] = (stream * scale * ffn_gain_ref[...]).astype(bf)

    first = {}

    def pack(k, target):
        picks = pick_ref[(z + k) % n_z]
        target[k, :, :width] = dot32(picks, normed_ref[...]).astype(bf)
        target[k, :, width:] = lax.dot_general(
            picks, info_ref[...], (((1,), (1,)), ((), ())), preferred_element_type=f32
        ).astype(bf)

    def launch(k):
        pack(k, out1)
        first[k] = remote(out1.at[k], in1.at[k], s1.at[k], r1.at[k], at_z(k))
        first[k].start()

    def slots(k):
        info = in1[k, :, width:].astype(f32)
        place = lax.broadcasted_iota(jnp.int32, (rows, peers * cap), 1).astype(f32)
        return place == info[:, 0:1], place == info[:, 1:2], info

    second = {}

    def scatter(k):
        if k:
            first[k].wait_recv()
        at0, at1, _ = slots(k)
        choose = (at0.astype(f32) + at1.astype(f32)).astype(bf)
        placed = dot_t(choose, in1[k, :, :width]).astype(bf)
        for e in range(peers):
            out2[k, e] = placed[e * cap : (e + 1) * cap]
        second[k] = [
            remote(
                out2.at[k, (mine + j) % peers], arrive.at[k, j], s2.at[k, j], r2.at[k, j], peer(j)
            )
            for j in range(1, peers)
        ]
        for copy in second[k]:
            copy.start()
        arrive[k, 0] = out2[k, mine]

    third = {}

    def serve(k):
        for copy in second[k]:
            copy.wait_recv()
        given = arrive[k].reshape(peers * cap, width)
        gate_act = dot32(given, gate_ref[...])
        upward = dot32(given, up_ref[...])
        hidden = (gate_act * (1.0 / (1.0 + jnp.exp(-gate_act))) * upward).astype(bf)
        result = dot32(hidden, down_ref[...]).astype(bf)
        for j in range(peers):
            served[k, j] = result[j * cap : (j + 1) * cap]
        third[k] = [
            remote(
                served.at[k, j], back2.at[k, mine], s3.at[k, j], r3.at[k, peers - j], peer(peers - j)
            )
            for j in range(1, peers)
        ]
        for copy in third[k]:
            copy.start()
        back2[k, mine] = served[k, 0]

    fourth = {}

    def merge(k):
        for copy in third[k]:
            copy.wait_recv()
        at0, at1, info = slots(k)
        high = jnp.where(at0, info[:, 2:3], 0.0) + jnp.where(at1, info[:, 4:5], 0.0)
        low = jnp.where(at0, info[:, 3:4], 0.0) + jnp.where(at1, info[:, 5:6], 0.0)
        got = back2[k].reshape(peers * cap, width)
        total = dot32(high.astype(bf), got) + dot32(low.astype(bf), got)
        if k:
            merged[k] = total.astype(bf)
            fourth[k] = remote(merged.at[k], home.at[k], s4.at[k], r4.at[k], at_z(n_z - k))
            fourth[k].start()
        else:
            acc[...] += dot_t(pick_ref[z], total.astype(bf))

    pack(0, in1)
    launch(1)
    scatter(0)
    launch(3)
    launch(2)
    for k in (1, 3, 2):
        scatter(k)
    def settle(copies):
        for copy in copies:
            copy.wait_send()

    for k in (1, 3, 2):
        serve(k)
    settle(list(down.values()) + list(over.values()) + sent + asked + list(first.values()))
    serve(0)
    settle(second[0] + second[1] + second[3] + second[2])
    for k in (1, 3, 2):
        merge(k)
    settle(third[1] + third[3])
    merge(0)
    for k in (1, 3, 2):
        fourth[k].wait_recv()
        acc[...] += dot_t(pick_ref[(z + k) % n_z], home[k])
    out_ref[...] = acc[...].astype(bf)
    settle(third[2] + third[0] + list(fourth.values()))


def selector(rows, columns, slot, source):
    head, lane = np.divmod(np.arange(columns), slot)
    origin = np.asarray([source(h, c) for h, c in zip(head, lane)])
    return (np.arange(rows)[:, None] == origin[None, :]).astype(jnp.bfloat16)


def selectors(heads, nope, rope, slot):
    qk = nope + rope
    half = rope // 2

    def swapped(c):
        return c + half if nope <= c < nope + half else c - half if nope + half <= c < qk else -1

    def plain(h, c):
        return c + h * qk if c < qk else -1

    def turned(h, c):
        return swapped(c) + h * qk if nope <= c < qk else -1

    def shared(h, c):
        return -1 if c < nope or c >= qk else (swapped(c) if h else c) - nope

    query = np.concatenate(
        [
            selector(heads * qk, heads * slot, slot, plain),
            selector(heads * qk, heads * slot, slot, turned),
        ],
        axis=1,
    )
    key = selector(
        heads * nope, heads * slot, slot, lambda h, c: c + h * nope if c < nope else -1
    )
    return query, key, selector(rope, 2 * slot, slot, shared)


def trig(positions, nope, rope):
    frequency = 10000.0 ** (-2.0 * np.arange(rope // 2) / rope)
    angle = np.asarray(positions, np.float64)[:, None] * frequency[None, :]
    cos = np.ones((len(positions), 128))
    sin = np.zeros((len(positions), 128))
    cos[:, nope : nope + rope] = np.concatenate([np.cos(angle)] * 2, axis=1)
    sin[:, nope : nope + rope] = np.concatenate([np.sin(angle)] * 2, axis=1)
    return np.stack([cos, sin]).astype(np.float32)


def per_device(
    residual,
    query,
    latent,
    rope_key,
    latent_gain,
    query_gain,
    key_gain,
    key_weight,
    value_weight,
    mix_gain,
    out_weight,
    ffn_gain,
    expert_choice,
    group_prob,
    expert_prob,
    gate_weight,
    up_weight,
    down_weight,
):
    n_sp = lax.axis_size("sp")
    n_dp = lax.axis_size("dp")
    n_z = GROUPS
    n_y = n_sp // n_z
    tok, width = residual.shape[1:]
    rope = rope_key.shape[2]
    qk = query_gain.shape[0]
    nope = qk - rope
    lat = latent.shape[2]
    head_count = query.shape[2] // qk
    value_width = value_weight.shape[1] // head_count
    heads = head_count // n_z
    length = n_sp * tok
    half = rope // 2
    top = expert_choice.shape[2]
    peers = n_y * n_dp
    cap = tok // peers
    rows = tok // top
    hidden = gate_weight.shape[2]
    slot = 128
    wide_v = heads * value_width
    bf = jnp.bfloat16
    f32 = jnp.float32
    near = jnp.asarray(trig(np.arange(tok), nope, rope))
    far = jnp.asarray(trig(np.arange(n_sp) * tok, nope, rope))
    picks, spreads, ropes = [jnp.asarray(m) for m in selectors(heads, nope, rope, slot)]
    vmem = pltpu.VMEM
    hbm = pl.BlockSpec(memory_space=pl.ANY)
    dma = pltpu.SemaphoreType.DMA
    out = pl.pallas_call(
        functools.partial(
            layer_kernel, n_sp, n_y, n_dp, nope, rope, value_width, cap, top
        ),
        out_shape=jax.ShapeDtypeStruct((tok, width), bf),
        in_specs=[hbm] * 23,
        out_specs=pl.BlockSpec(memory_space=vmem),
        scratch_shapes=[
            vmem((tok, width), bf),
            vmem((tok, lat), bf),
            vmem((rope, tok), bf),
            vmem((1, lat), f32),
            vmem((1, qk), f32),
            vmem((1, qk), f32),
            vmem((lat, wide_v), bf),
            vmem((lat, wide_v), bf),
            vmem((1, head_count * value_width), f32),
            vmem(out_weight.shape, bf),
            vmem((1, width), f32),
            vmem((top, tok), jnp.int32),
            vmem((1, tok), f32),
            vmem((top, tok), f32),
            vmem((width, hidden), bf),
            vmem((width, hidden), bf),
            vmem((hidden, width), bf),
            vmem(near.shape, f32),
            vmem(far.shape, f32),
            vmem((lat, heads * slot), bf),
            vmem(picks.shape, bf),
            vmem(spreads.shape, bf),
            vmem(ropes.shape, bf),
            vmem((n_z, tok, heads * qk), bf),
            vmem((tok + half, lat), bf),
            vmem((n_sp, tok + half, lat), bf),
            vmem((n_z, heads, tok, slot), bf),
            vmem((heads, length, slot), bf),
            vmem((length, wide_v), bf),
            vmem((tok, n_y * tok), f32),
            vmem((heads * tok, length), bf),
            vmem((n_z, tok, wide_v), bf),
            vmem((n_z, tok, wide_v), bf),
            vmem((tok, width), bf),
            vmem((slot, tok), bf),
            vmem((n_z, rows, tok), bf),
            vmem((n_z, rows, width + slot), bf),
            vmem((n_z, rows, width + slot), bf),
            vmem((n_z, peers, cap, width), bf),
            vmem((n_z, peers, cap, width), bf),
            vmem((n_z, peers, cap, width), bf),
            vmem((n_z, peers, cap, width), bf),
            vmem((n_z, rows, width), bf),
            vmem((n_z, rows, width), bf),
            vmem((tok, width), f32),
            dma((23,)),
            dma((n_z,)),
            dma((n_z,)),
            dma((n_z,)),
            dma((n_z,)),
            dma((n_y,)),
            dma((n_y,)),
            dma((n_z, n_y)),
            dma((n_z, n_y)),
            dma((n_y, n_z)),
            dma((n_y, n_z)),
            dma((n_z,)),
            dma((n_z,)),
            dma((n_z,)),
            dma((n_z,)),
            dma((n_z, peers)),
            dma((n_z, peers)),
            dma((n_z, peers)),
            dma((n_z, peers)),
            dma((n_z,)),
            dma((n_z,)),
        ],
        compiler_params=pltpu.CompilerParams(
            collective_id=0, has_side_effects=True, vmem_limit_bytes=50 * 1024 * 1024
        ),
    )(
        *[pltpu.with_memory_space_constraint(v, pltpu.HBM) for v in (residual[0],
        query[0],
        latent[0],
        rope_key[0].T,
        latent_gain[None],
        query_gain[None],
        key_gain[None],
        key_weight,
        value_weight,
        mix_gain[None],
        out_weight,
        ffn_gain[None],
        expert_choice[0].T,
        group_prob,
        expert_prob[0].T,
        gate_weight[0],
        up_weight[0],
        down_weight[0],
        near,
        far,
        picks,
        spreads,
        ropes)],
    )
    return out[None]


def solution(mesh):
    return jax.shard_map(
        per_device,
        mesh=mesh,
        in_specs=(
            P("dp", "sp", None),
            P("dp", "sp", None),
            P("dp", "sp", None),
            P("dp", "sp", None),
            P(),
            P(),
            P(),
            P(),
            P(),
            P(),
            P(),
            P(),
            P("dp", "sp", None),
            P("dp", "sp"),
            P("dp", "sp", None),
            P(("sp", "dp"), None, None),
            P(("sp", "dp"), None, None),
            P(("sp", "dp"), None, None),
        ),
        out_specs=P("dp", "sp", None),
        check_vma=False,
    )
```
